32 devices in a mesh: sp: 8 (over z, y), tp: 4 (over x, core).
Axes of the slice: x: 2, y: 2, z: 4, core: 2. Of those that a mesh axis runs over, the one named last changes fastest.
Arguments:
- resid: bfloat16 [1536, 2048], P('sp'), may hold values from -6 to 6
- query_broad: bfloat16 [1536, 1536], P('sp', 'tp'), may hold values from -60 to 60
- query_narrow: bfloat16 [1536, 1024], P('sp', 'tp'), may hold values from -60 to 60
- latent: bfloat16 [1536, 512], P('sp'), may hold values from -6 to 6
- key_rope: bfloat16 [1536, 64], P('sp'), may hold values from -6 to 6
- latent_gain: float32 [512], replicated, may hold values from 0.1 to 1.9
- key_up_broad: bfloat16 [512, 1024], P(None, 'tp'), may hold values from -0.25 to 0.25
- value_up_broad: bfloat16 [512, 1024], P(None, 'tp'), may hold values from -0.25 to 0.25
- key_up_narrow: bfloat16 [512, 512], P(None, 'tp'), may hold values from -0.25 to 0.25
- value_up_narrow: bfloat16 [512, 512], P(None, 'tp'), may hold values from -0.25 to 0.25
- out_broad: bfloat16 [1024, 2048], replicated, may hold values from -0.15625 to 0.15625
- out_narrow: bfloat16 [512, 2048], replicated, may hold values from -0.15625 to 0.15625
- post_gain: float32 [2048], replicated, may hold values from 0.1 to 1.9
- ffn_gain: float32 [2048], replicated, may hold values from 0.1 to 1.9
- up_weight: bfloat16 [2048, 8192], P('sp', 'tp'), may hold values from -0.125 to 0.125
- down_weight: bfloat16 [2048, 8192], P('sp', 'tp'), may hold values from -0.0625 to 0.0625
- ffn_out_gain: float32 [2048], replicated, may hold values from 0.1 to 1.9
Outputs:
- layer_out: bfloat16 [1536, 2048], P(('sp', 'tp'))
The draws below stay inside these ranges and needn't reach their ends.
All inputs are finite; a program needn't handle non-finite values.
Results may differ from the reference program's by a relative error of at most 0.013.
Values may be sent and summed in bfloat16 or wider, within the bound.
A program may use at most 128 MiB of HBM per device.

```python
import math
import jax
import jax.numpy as jnp
from jax import lax

D = 2048
FF = 8192
R = 512
ROPE = 64
DB = 128
DN = 64
HB = 8
HN = 8
SEQ = 1536


def drawn_queries(key, salt, head_count, head_size):
    drawn = jax.random.normal(jax.random.fold_in(key, salt), (SEQ, head_count, head_size + ROPE), jnp.float32)
    return jnp.clip(drawn, -6.0, 6.0)


def draw_query_broad(key, part):
    entries = drawn_queries(key, 21, HB, DB)
    return entries.reshape(SEQ, HB * (DB + ROPE)).astype(jnp.bfloat16)


def draw_query_narrow(key, part):
    entries = drawn_queries(key, 31, HN, DN)
    return entries.reshape(SEQ, HN * (DN + ROPE)).astype(jnp.bfloat16)


def draw_key_rope(key, part):
    entries = jnp.clip(jax.random.normal(jax.random.fold_in(key, 11), (SEQ, ROPE), jnp.float32), -6.0, 6.0)
    return entries.astype(jnp.bfloat16)


def block_scale(rng, dims, cuts, least, top_value):
    def one(dim, shards_of):
        heights = jax.random.uniform(jax.random.fold_in(jax.random.fold_in(rng, 6), dim), (shards_of,), jnp.float32, least / len(cuts), top_value / len(cuts))
        return jnp.repeat(jnp.exp(heights), dims[dim] // shards_of).reshape((-1,) + (1,) * (len(dims) - dim - 1))

    factor_of = one(*cuts[0])
    for cut in cuts[1:]:
        factor_of = factor_of * one(*cut)
    return factor_of


def bell_draw(rng, extent, width, reach, cuts=(), held_as=jnp.bfloat16):
    factor_of = block_scale(rng, extent, cuts, -0.22, 0.18) if cuts else 1.0
    result = jax.random.normal(rng, extent, jnp.float32) * width * factor_of
    return jnp.minimum(jnp.maximum(result, -reach), reach).astype(held_as)


def setup_inputs(seed: int = 0) -> dict:
    streams_of = jax.random.split(jax.random.key(seed), 18)
    return {
        "resid": bell_draw(streams_of[0], (SEQ, D), 1.0, 6.0, ((0, 8),)),
        "query_broad": draw_query_broad(jax.random.fold_in(streams_of[17], 71), 0),
        "query_narrow": draw_query_narrow(jax.random.fold_in(streams_of[17], 71), 0),
        "latent": bell_draw(streams_of[3], (SEQ, R), 1.0, 6.0, ((0, 8),)),
        "key_rope": draw_key_rope(jax.random.fold_in(streams_of[17], 71), 0),
        "latent_gain": jnp.clip(1.0 + 0.18 * jax.random.normal(streams_of[5], (R,), jnp.float32), 0.1, 1.9),
        "key_up_broad": bell_draw(streams_of[6], (R, HB * DB), R ** -0.5, 0.25, ((1, 4),)),
        "value_up_broad": bell_draw(streams_of[7], (R, HB * DB), R ** -0.5, 0.25, ((1, 4),)),
        "key_up_narrow": bell_draw(streams_of[8], (R, HN * DN), R ** -0.5, 0.25, ((1, 4),)),
        "value_up_narrow": bell_draw(streams_of[9], (R, HN * DN), R ** -0.5, 0.25, ((1, 4),)),
        "out_broad": bell_draw(streams_of[10], (HB * DB, D), (HB * DB + HN * DN) ** -0.5, 0.15625),
        "out_narrow": bell_draw(streams_of[11], (HN * DN, D), (HB * DB + HN * DN) ** -0.5, 0.15625),
        "post_gain": jnp.clip(1.0 + 0.18 * jax.random.normal(streams_of[12], (D,), jnp.float32), 0.1, 1.9),
        "ffn_gain": jnp.clip(1.0 + 0.18 * jax.random.normal(streams_of[13], (D,), jnp.float32), 0.1, 1.9),
        "up_weight": bell_draw(streams_of[14], (D, FF), D ** -0.5, 0.125, ((0, 8), (1, 4))),
        "down_weight": bell_draw(streams_of[15], (D, FF), FF ** -0.5, 0.0625, ((0, 8), (1, 4))),
        "ffn_out_gain": jnp.clip(1.0 + 0.18 * jax.random.normal(streams_of[16], (D,), jnp.float32), 0.1, 1.9),
    }


norm_eps = 1e-06
rope_base = 500000.0
masked_score = -1e+30

def rotate(values, positions):
    full_width = values.shape[-1]
    half_width = full_width // 2
    frequency = rope_base ** (-2.0 * jnp.arange(half_width, dtype=jnp.float32) / full_width)
    angles = positions.astype(jnp.float32)[:, None] * frequency[None, :]
    angle_shape = (angles.shape[0],) + (1,) * (values.ndim - 2) + (half_width,)
    cosine = jnp.cos(angles).reshape(angle_shape)
    sine_part = jnp.sin(angles).reshape(angle_shape)
    leading = values[..., :half_width]
    trailing = values[..., half_width:]
    return jnp.concatenate([leading * cosine - trailing * sine_part, trailing * cosine + leading * sine_part], axis=-1)

def rms_scale(values, norm_gain):
    return values * lax.rsqrt(lax.optimization_barrier(jnp.mean(values * values, axis=-1, keepdims=True)) + norm_eps) * norm_gain

def attend_all(query_nope, query_rope, key_rows, key_rot, value_rows, score_scale):
    block_rows = math.gcd(SEQ, 512)
    positions = jnp.arange(SEQ, dtype=jnp.int32)
    keys_wide = key_rows.astype(jnp.float32)
    rot_wide = key_rot.astype(jnp.float32)
    values_wide = value_rows.astype(jnp.float32)

    def one_block(block_index):
        begin = block_index * block_rows
        nope_part = lax.dynamic_slice_in_dim(query_nope, begin, block_rows, 0).astype(jnp.float32)
        rope_part = lax.dynamic_slice_in_dim(query_rope, begin, block_rows, 0).astype(jnp.float32)
        query_pos = begin + jnp.arange(block_rows, dtype=jnp.int32)
        scores = jnp.einsum('qhd,khd->hqk', nope_part, keys_wide) + jnp.einsum('qhd,kd->hqk', rope_part, rot_wide)
        scores = scores * score_scale
        allowed = (positions[None, :] <= query_pos[:, None])[None]
        scores = jnp.where(allowed, scores, masked_score)
        highest = lax.optimization_barrier(jnp.max(scores, axis=-1, keepdims=True))
        exponent = jnp.where(allowed, jnp.exp(scores - highest), 0.0)
        denominator = lax.optimization_barrier(jnp.sum(exponent, axis=-1))
        rounded = lax.optimization_barrier(exponent.astype(jnp.bfloat16)).astype(jnp.float32)
        summed = jnp.einsum('hqk,khd->qhd', rounded, values_wide)
        return (summed / jnp.transpose(denominator)[:, :, None]).astype(jnp.bfloat16)
    heads_out = lax.map(one_block, jnp.arange(SEQ // block_rows, dtype=jnp.int32))
    return heads_out.reshape(SEQ, value_rows.shape[1] * value_rows.shape[2])

def reference(resid, query_broad, query_narrow, latent, key_rope, latent_gain, key_up_broad, value_up_broad, key_up_narrow, value_up_narrow, out_broad, out_narrow, post_gain, ffn_gain, up_weight, down_weight, ffn_out_gain):
    positions = jnp.arange(SEQ, dtype=jnp.int32)
    latent_normed = rms_scale(latent.astype(jnp.float32), latent_gain).astype(jnp.bfloat16)

    def expand(weight, head_size):
        product = jnp.dot(latent_normed, weight, preferred_element_type=jnp.float32)
        return product.astype(jnp.bfloat16).reshape(SEQ, -1, head_size)
    key_broad = expand(key_up_broad, DB)
    value_broad = expand(value_up_broad, DB)
    key_narrow = expand(key_up_narrow, DN)
    value_narrow = expand(value_up_narrow, DN)
    key_rot = rotate(key_rope.astype(jnp.float32), positions).astype(jnp.bfloat16)
    broad_heads = query_broad.reshape(SEQ, HB, DB + ROPE)
    broad_rope = rotate(broad_heads[:, :, DB:].astype(jnp.float32), positions).astype(jnp.bfloat16)
    narrow_heads = query_narrow.reshape(SEQ, HN, DN + ROPE)
    narrow_rope = rotate(narrow_heads[:, :, DN:].astype(jnp.float32), positions).astype(jnp.bfloat16)
    attn_broad = attend_all(broad_heads[:, :, :DB], broad_rope, key_broad, key_rot, value_broad, (DB + ROPE) ** (-0.5))
    attn_narrow = attend_all(narrow_heads[:, :, :DN], narrow_rope, key_narrow, key_rot, value_narrow, (DN + ROPE) ** (-0.5))
    projected = jnp.dot(attn_broad, out_broad, preferred_element_type=jnp.float32) + jnp.dot(attn_narrow, out_narrow, preferred_element_type=jnp.float32)
    mixed = (resid.astype(jnp.float32) + rms_scale(projected, post_gain)).astype(jnp.bfloat16)
    normed = rms_scale(mixed.astype(jnp.float32), ffn_gain).astype(jnp.bfloat16)
    hidden = jnp.square(jax.nn.relu(jnp.dot(normed, up_weight, preferred_element_type=jnp.float32))).astype(jnp.bfloat16)
    ffn = lax.dot_general(hidden, down_weight, (((1,), (1,)), ((), ())), preferred_element_type=jnp.float32)
    return (mixed.astype(jnp.float32) + rms_scale(ffn, ffn_out_gain)).astype(jnp.bfloat16)
```

```python
import functools
import math

import jax
import jax.numpy as jnp
from jax import lax
from jax.experimental import pallas as pl
from jax.experimental.pallas import tpu as pltpu
from jax.sharding import PartitionSpec as P

DB = 128
DN = 64


norm_eps = 1e-06
rope_base = 500000.0
masked_score = -1e30


def rotate(values, positions):
    full_width = values.shape[-1]
    half_width = full_width // 2
    frequency = rope_base ** (-2.0 * jnp.arange(half_width, dtype=jnp.float32) / full_width)
    angles = positions.astype(jnp.float32)[:, None] * frequency[None, :]
    angle_shape = (angles.shape[0],) + (1,) * (values.ndim - 2) + (half_width,)
    cosine = jnp.cos(angles).reshape(angle_shape)
    sine_part = jnp.sin(angles).reshape(angle_shape)
    leading = values[..., :half_width]
    trailing = values[..., half_width:]
    return jnp.concatenate(
        [leading * cosine - trailing * sine_part, trailing * cosine + leading * sine_part], axis=-1
    )


def rms_scale(values, norm_gain):
    return (
        values * lax.rsqrt(jnp.mean(values * values, axis=-1, keepdims=True) + norm_eps) * norm_gain
    )


def group_update(
    running, nope_query, rope_query, key_rows, key_rot, value_rows, score_scale, allowed
):
    old_max, old_sum, old_acc = running
    scores = jnp.einsum("qhd,khd->hqk", nope_query, key_rows, preferred_element_type=jnp.float32)
    scores = scores + jnp.einsum(
        "qhd,kd->hqk", rope_query, key_rot, preferred_element_type=jnp.float32
    )
    scores = jnp.where(allowed, scores * score_scale, masked_score)
    new_max = jnp.maximum(old_max, jnp.max(scores, axis=-1))
    exponent = jnp.where(allowed, jnp.exp(scores - new_max[:, :, None]), 0.0)
    factor = jnp.exp(old_max - new_max)
    new_sum = old_sum * factor + jnp.sum(exponent, axis=-1)
    weighted = jnp.einsum(
        "hqk,khd->qhd",
        exponent.astype(jnp.bfloat16),
        value_rows,
        preferred_element_type=jnp.float32,
    )
    new_acc = old_acc * jnp.transpose(factor)[:, :, None] + weighted
    return (new_max, new_sum, new_acc)


def local(
    resid,
    query_broad,
    query_narrow,
    latent,
    key_rope,
    latent_gain,
    key_up_broad,
    value_up_broad,
    key_up_narrow,
    value_up_narrow,
    out_broad,
    out_narrow,
    post_gain,
    ffn_gain,
    up_weight,
    down_weight,
    ffn_out_gain,
):
    local_rows = resid.shape[0]
    head_parts = lax.axis_size("tp")
    share_rows = local_rows // head_parts
    row_offset = lax.axis_index("sp") * local_rows
    last_query = row_offset + local_rows - 1
    query_pos = row_offset + jnp.arange(local_rows, dtype=jnp.int32)
    rope_width = key_rope.shape[1]
    broad_count = key_up_broad.shape[1] // DB
    narrow_count = key_up_narrow.shape[1] // DN
    broad_heads = query_broad.reshape(local_rows, broad_count, DB + rope_width)
    broad_nope = broad_heads[:, :, :DB]
    broad_rope = rotate(broad_heads[:, :, DB:].astype(jnp.float32), query_pos).astype(jnp.bfloat16)
    narrow_heads = query_narrow.reshape(local_rows, narrow_count, DN + rope_width)
    narrow_nope = narrow_heads[:, :, :DN]
    narrow_rope = rotate(narrow_heads[:, :, DN:].astype(jnp.float32), query_pos).astype(
        jnp.bfloat16
    )
    broad_scale = (DB + rope_width) ** (-0.5)
    narrow_scale = (DN + rope_width) ** (-0.5)

    def attend(running, latent_rows, rope_rows, first_row):
        key_count = latent_rows.shape[0]
        key_pos = first_row + jnp.arange(key_count, dtype=jnp.int32)
        latent_normed = rms_scale(latent_rows.astype(jnp.float32), latent_gain).astype(jnp.bfloat16)

        def expand(weight, head_size):
            product = jnp.dot(latent_normed, weight, preferred_element_type=jnp.float32)
            return product.astype(jnp.bfloat16).reshape(key_count, -1, head_size)

        key_rot = rotate(rope_rows.astype(jnp.float32), key_pos).astype(jnp.bfloat16)
        allowed = (key_pos[None, :] <= query_pos[:, None])[None]
        broad_state = group_update(
            running[0],
            broad_nope,
            broad_rope,
            expand(key_up_broad, DB),
            key_rot,
            expand(value_up_broad, DB),
            broad_scale,
            allowed,
        )
        narrow_state = group_update(
            running[1],
            narrow_nope,
            narrow_rope,
            expand(key_up_narrow, DN),
            key_rot,
            expand(value_up_narrow, DN),
            narrow_scale,
            allowed,
        )
        return (broad_state, narrow_state)

    def fresh(head_count, head_size):
        return (
            jnp.full((head_count, local_rows), masked_score, jnp.float32),
            jnp.zeros((head_count, local_rows), jnp.float32),
            jnp.zeros((local_rows, head_count, head_size), jnp.float32),
        )

    initial = (fresh(broad_count, DB), fresh(narrow_count, DN))
    latent_piece = lax.all_gather(latent, "sp", axis=0, tiled=True)
    rope_piece = lax.all_gather(key_rope, "sp", axis=0, tiled=True)
    piece_rows = latent_piece.shape[0]
    block_rows = math.gcd(piece_rows, 1024)

    def one_block(block_index, carried):
        begin = block_index * block_rows
        latent_block = lax.dynamic_slice_in_dim(latent_piece, begin, block_rows, 0)
        rope_block = lax.dynamic_slice_in_dim(rope_piece, begin, block_rows, 0)

        def unchanged(kept_state):
            return kept_state

        def updated(kept_state):
            return attend(kept_state, latent_block, rope_block, begin)

        return lax.cond(begin > last_query, unchanged, updated, carried)

    final_state = lax.fori_loop(0, piece_rows // block_rows, one_block, initial)

    def finish(running):
        run_max, run_sum, run_acc = running
        return (
            (run_acc / jnp.transpose(run_sum)[:, :, None])
            .astype(jnp.bfloat16)
            .reshape(local_rows, -1)
        )

    attn_broad = finish(final_state[0])
    attn_narrow = finish(final_state[1])
    rows_broad, rows_narrow = (
        lax.all_to_all(attn_broad, "tp", split_axis=0, concat_axis=1, tiled=True),
        lax.all_to_all(attn_narrow, "tp", split_axis=0, concat_axis=1, tiled=True),
    )
    projected = jnp.dot(rows_broad, out_broad, preferred_element_type=jnp.float32) + jnp.dot(
        rows_narrow, out_narrow, preferred_element_type=jnp.float32
    )
    own_resid = lax.dynamic_slice_in_dim(resid, lax.axis_index("tp") * share_rows, share_rows, 0)
    mixed = (own_resid.astype(jnp.float32) + rms_scale(projected, post_gain)).astype(jnp.bfloat16)
    normed = rms_scale(mixed.astype(jnp.float32), ffn_gain).astype(jnp.bfloat16)
    up_full, down_full = (
        lax.all_gather(up_weight, "sp", axis=0, tiled=True),
        lax.all_gather(down_weight, "sp", axis=0, tiled=True),
    )
    hidden = jnp.square(
        jax.nn.relu(
            jnp.dot(
                lax.all_gather(normed, "tp", axis=0, tiled=True),
                up_full,
                preferred_element_type=jnp.float32,
            )
        )
    ).astype(jnp.bfloat16)
    ffn = lax.psum_scatter(
        lax.dot_general(
            hidden, down_full, (((1,), (1,)), ((), ())), preferred_element_type=jnp.float32
        ).astype(jnp.bfloat16),
        "tp",
        scatter_dimension=0,
        tiled=True,
    ).astype(jnp.float32)
    return (mixed.astype(jnp.float32) + rms_scale(ffn, ffn_out_gain)).astype(jnp.bfloat16)

lane_tile = 128
row_parts = 2
mesh_id = pl.DeviceIdType.MESH


def sem_layout(lines, tp, chunks):
    sizes = {
        "lat_z": lines,
        "lat_y": lines,
        "lat_x": 2 * lines,
        "lat_c": 4 * lines,
        "up_z": lines,
        "up_y": lines,
        "up_c": 2 * lines,
        "down_z": 2 * lines,
        "down_y": 2 * lines,
        "down_c": 4 * lines,
        "heads": tp,
        "row_z": lines,
        "row_x": lines,
        "sum_x": chunks * lines,
        "sum_r": chunks * 2,
        "sum_m": chunks,
        "sum_f": chunks,
    }
    base, total = {}, 0
    for name, size in sizes.items():
        base[name] = total
        total += size
    return base, total


def layer_kernel(
    sp,
    tp,
    latent_ref,
    key_rope_ref,
    table_ref,
    latent_gain_ref,
    qb_in,
    qn_in,
    resid_ref,
    kb_ref,
    vb_ref,
    kn_ref,
    vn_ref,
    ob_hbm,
    on_hbm,
    post_ref,
    gain_ref,
    last_ref,
    up_hbm,
    down_hbm,
    out_ref,
    mine_ref,
    qb_ref,
    qn_ref,
    lat,
    top_ref,
    sum_ref,
    acc_ref,
    attn,
    heads,
    ob,
    on,
    up,
    down,
    rows,
    hidden_ref,
    part,
    x_send,
    x_got,
    z_send,
    r_got,
    m_got,
    f_got,
    ffn_ref,
    send_sem,
    recv_sem,
    local_sem,
):
    cols = row_parts
    lines = sp // cols
    chunks = 4
    s = lax.axis_index("sp")
    t = lax.axis_index("tp")
    z = s // cols
    y = s % cols
    core = t % 2
    x = t // 2
    t_core = 2 * x + 1 - core
    t_x = 2 * (1 - x) + core
    t_both = 2 * (1 - x) + 1 - core
    s_y = z * cols + 1 - y
    half = z // 2
    mate = z + 1 - 2 * (z % 2)
    gate = 2 - half
    outer = 3 * (1 - half)
    inner = (z == 1) | (z == 2)
    edge = (z == 0) | (z == 3)
    bf16 = jnp.bfloat16
    f32 = jnp.float32
    share = resid_ref.shape[0] // tp
    block_rows = resid_ref.shape[0]
    width = up.shape[3]
    piece = down.shape[4]
    base, _ = sem_layout(lines, tp, chunks)

    def line(at):
        return (at * cols + y, t)

    peer_y, peer_x, peer_c, peer_b = (s_y, t), (s, t_x), (s, t_core), (s, t_both)
    peers = [line(mate), line(gate), line(outer), peer_y, peer_x, peer_c, peer_b]
    barrier = pltpu.get_barrier_semaphore()
    for peer in peers:
        pl.semaphore_signal(barrier, inc=1, device_id=peer, device_id_type=mesh_id)

    rope = key_rope_ref.shape[1]
    half_rope = rope // 2

    def turn(values, table):
        values = values.astype(f32)
        swapped = jnp.concatenate([values[:, half_rope:], values[:, :half_rope]], axis=1)
        return (values * table[:, :rope] + swapped * table[:, rope:]).astype(bf16)

    latent_width = latent_ref.shape[1]
    mine_rows = pl.ds(pl.multiple_of(t * share, 16), share)
    mine_ref[:, :latent_width] = rms_scale(
        latent_ref[mine_rows, :].astype(f32), latent_gain_ref[...]
    ).astype(bf16)
    mine_ref[:, latent_width:] = turn(key_rope_ref[mine_rows, :], table_ref[mine_rows, :])
    pl.semaphore_wait(barrier, len(peers))

    started = []

    def send(src, dst, peer, recv, cond=None):
        copy = pltpu.make_async_remote_copy(
            src_ref=src,
            dst_ref=dst,
            send_sem=send_sem.at[len(started)],
            recv_sem=recv_sem.at[recv],
            device_id=peer,
            device_id_type=mesh_id,
        )
        started.append((cond, copy))
        if cond is None:
            copy.start()
        else:
            pl.when(cond)(lambda: copy.start())

    def arrive(dst, recv):
        pltpu.make_async_remote_copy(
            src_ref=dst,
            dst_ref=dst,
            send_sem=send_sem.at[0],
            recv_sem=recv_sem.at[recv],
            device_id=peer_c,
            device_id_type=mesh_id,
        ).wait_recv()

    locals_ = []

    def bring(src, dst):
        copy = pltpu.make_async_copy(src, dst, local_sem.at[len(locals_)])
        copy.start()
        locals_.append(copy)
        return copy

    def block(k, flipped):
        return (z - k) * cols + ((1 - y) if flipped else y)

    for k in range(1, lines):
        send(mine_ref, lat.at[s, t], line(z + k), base["lat_z"] + k, z + k < lines)
    send(mine_ref, lat.at[s, t], peer_y, base["lat_y"])
    send(mine_ref, lat.at[s, t], peer_x, base["lat_x"])
    send(mine_ref, lat.at[s, t], peer_c, base["lat_c"])
    own_copy = bring(mine_ref, lat.at[s, t])

    def cut(ref, at, first=0, count=None):
        columns = pl.ds(pl.multiple_of(at * width, width), width)
        return ref.at[pl.ds(first, ref.shape[0] if count is None else count), columns]

    far = (gate, outer, mate)

    def up_at(origin, at):
        return up.at[origin, at]

    def down_at(origin, at, upper):
        return down.at[origin, at // cols, at % cols, upper]

    def send_down(upper):
        for dest in far:
            send(
                cut(down_hbm, dest, upper * piece, piece),
                down_at(core, s, upper),
                line(dest),
                base["down_z"] + upper * lines + z,
            )

    for dest in far:
        send(cut(up_hbm, dest), up_at(core, s), line(dest), base["up_z"] + z)
    own = [bring(cut(up_hbm, z), up_at(core, s))]
    for upper in range(2):
        own.append(
            bring(cut(down_hbm, z, upper * piece, piece), down_at(core, s, upper))
        )
    outs = [bring(ob_hbm, ob), bring(on_hbm, on)]

    for queries, turned, size in ((qb_in, qb_ref, DB), (qn_in, qn_ref, DN)):
        step = size + rope
        for h in range(queries.shape[1] // step):
            middle = h * step + size
            turned[:, h * step : middle] = queries[:, h * step : middle]
            turned[:, middle : middle + rope] = turn(
                queries[:, middle : middle + rope], table_ref[...]
            )

    def when(k):
        return None if k == 0 else z >= k

    def guarded(k, body):
        if k == 0:
            body()
        else:
            pl.when(z >= k)(body)

    def lat_in_z(k):
        held = lat.at[block(k, False), t]
        guarded(k, lambda: arrive(held, base["lat_z"] + k))
        send(held, held, peer_y, base["lat_y"] + k, when(k))
        send(held, held, peer_x, base["lat_x"] + 2 * k, when(k))
        send(held, held, peer_c, base["lat_c"] + 4 * k, when(k))

    def lat_in_y(k):
        held = lat.at[block(k, True), t]
        guarded(k, lambda: arrive(held, base["lat_y"] + k))
        send(held, held, peer_x, base["lat_x"] + 2 * k + 1, when(k))
        send(held, held, peer_c, base["lat_c"] + 4 * k + 1, when(k))

    def lat_in_x(k):
        for i, flipped in enumerate((False, True)):
            held = lat.at[block(k, flipped), t_x]
            guarded(k, lambda: arrive(held, base["lat_x"] + 2 * k + i))
            send(held, held, peer_c, base["lat_c"] + 4 * k + 2 + i, when(k))

    broad = kb_ref.shape[1] // DB
    narrow = kn_ref.shape[1] // DN
    wb = DB + rope
    wn = DN + rope
    keys = cols * block_rows

    def attend(k):
        for i, flipped in enumerate((False, True)):
            arrive(lat.at[block(k, flipped), t_core], base["lat_c"] + 4 * k + i)
            arrive(lat.at[block(k, flipped), t_both], base["lat_c"] + 4 * k + 2 + i)
        both = lat[pl.ds((z - k) * cols, cols)].reshape(keys, latent_width + rope)
        normed = both[:, :latent_width]
        rot = both[:, latent_width:]

        def expand(ref):
            return jnp.dot(normed, ref[...], preferred_element_type=f32).astype(bf16)

        kb, vb, kn, vn = expand(kb_ref), expand(vb_ref), expand(kn_ref), expand(vn_ref)
        if k == 0:
            query_pos = y * block_rows + lax.broadcasted_iota(jnp.int32, (block_rows, keys), 0)
            allowed = lax.broadcasted_iota(jnp.int32, (block_rows, keys), 1) <= query_pos
        for h in range(broad + narrow):
            if h < broad:
                q = qb_ref[:, h * wb : (h + 1) * wb]
                key = jnp.concatenate([kb[:, h * DB : (h + 1) * DB], rot], axis=1)
                v = vb[:, h * DB : (h + 1) * DB]
                scale = wb ** (-0.5)
            else:
                n = h - broad
                q = qn_ref[:, n * wn : (n + 1) * wn]
                key = jnp.concatenate([kn[:, n * DN : (n + 1) * DN], rot], axis=1)
                v = vn
                scale = wn ** (-0.5)
            score = scale * lax.dot_general(
                q, key, (((1,), (1,)), ((), ())), preferred_element_type=f32
            )
            if k == 0:
                score = jnp.where(allowed, score, masked_score)
                new_max = jnp.max(score, axis=-1, keepdims=True)
                e = jnp.where(allowed, jnp.exp(score - new_max), 0.0)
                new_sum = jnp.sum(e, axis=-1, keepdims=True)
                acc_ref[h] = jnp.dot(e.astype(bf16), v, preferred_element_type=f32)
            else:
                old_max = top_ref[h]
                new_max = jnp.maximum(old_max, jnp.max(score, axis=-1, keepdims=True))
                e = jnp.exp(score - new_max)
                factor = jnp.exp(old_max - new_max)
                new_sum = sum_ref[h] * factor + jnp.sum(e, axis=-1, keepdims=True)
                acc_ref[h] = acc_ref[h] * factor + jnp.dot(
                    e.astype(bf16), v, preferred_element_type=f32
                )
            top_ref[h] = new_max
            sum_ref[h] = new_sum

    lat_in_y(0)
    lat_in_x(0)
    lat_in_z(1)
    own_copy.wait()
    attend(0)
    lat_in_y(1)
    lat_in_x(1)
    lat_in_z(2)
    lat_in_z(3)
    guarded(1, lambda: attend(1))
    lat_in_y(2)
    lat_in_y(3)
    send(cut(up_hbm, z), up_at(core, s), peer_y, base["up_y"])
    lat_in_x(2)
    lat_in_x(3)
    send(cut(up_hbm, z), up_at(core, s), peer_c, base["up_c"])
    guarded(2, lambda: attend(2))
    guarded(3, lambda: attend(3))

    parts = [acc_ref[h] / sum_ref[h] for h in range(broad + narrow)]
    for h in range(broad):
        for i in range(tp):
            attn[i, :, h * DB : (h + 1) * DB] = parts[h][i * share : (i + 1) * share].astype(bf16)
    column = lax.broadcasted_iota(jnp.int32, parts[broad].shape, 1)
    merged = parts[broad]
    for n in range(1, narrow):
        merged = jnp.where(column >= n * DN, parts[broad + n], merged)
    for i in range(tp):
        attn[i, :, broad * DB :] = merged[i * share : (i + 1) * share].astype(bf16)

    turned_to = ((t_x, peer_x), (t_both, peer_b), (t_core, peer_c))
    for i, (at, peer) in enumerate(turned_to):
        send(attn.at[at], heads.at[t], peer, base["heads"] + i)
    heads[t] = attn[t]
    for upper in range(2):
        send(
            cut(down_hbm, z, upper * piece, piece),
            down_at(core, s, upper),
            peer_y,
            base["down_y"] + upper * lines,
        )
        send(
            cut(down_hbm, z, upper * piece, piece),
            down_at(core, s, upper),
            peer_c,
            base["down_c"] + upper * 2 * lines,
        )
    for copy in outs:
        copy.wait()
    for i, (at, _) in enumerate(turned_to):
        arrive(heads.at[at], base["heads"] + i)

    broad_width = kb_ref.shape[1]
    narrow_width = kn_ref.shape[1]
    projected = jnp.zeros((share, ob.shape[1]), f32)
    for i in range(tp):
        projected = projected + jnp.dot(
            heads[i, :, :broad_width],
            ob[i * broad_width : (i + 1) * broad_width],
            preferred_element_type=f32,
        )
        projected = projected + jnp.dot(
            heads[i, :, broad_width:],
            on[i * narrow_width : (i + 1) * narrow_width],
            preferred_element_type=f32,
        )
    mixed = (
        resid_ref[pl.ds(pl.multiple_of(t * share, 16), share), :].astype(f32)
        + rms_scale(projected, post_ref[...])
    ).astype(bf16)
    rows[0, z] = rms_scale(mixed.astype(f32), gain_ref[...]).astype(bf16)

    held = rows.at[0, z]
    send(held, held, line(gate), base["row_z"] + z)
    send(held, held, line(mate), base["row_z"] + z)
    send(held, rows.at[1, z], peer_x, base["row_x"])
    send_down(0)

    def up_in_z(i, at):
        held = up_at(core, at * cols + y)
        arrive(held, base["up_z"] + at)
        send(held, held, peer_y, base["up_y"] + 1 + i)
        send(held, held, peer_c, base["up_c"] + 1 + i)

    def up_in_y(i, at):
        held = up_at(core, at * cols + 1 - y)
        arrive(held, base["up_y"] + i)
        send(held, held, peer_c, base["up_c"] + lines + i)

    def row_in(i, at):
        held = rows.at[0, at]
        arrive(held, base["row_z"] + at)
        if i < 2:
            send(held, held, line(mate), base["row_z"] + at, inner)
        send(held, rows.at[1, at], peer_x, base["row_x"] + 1 + i)

    for i, at in enumerate(far):
        up_in_z(i, at)
    row_in(2, mate)
    row_in(0, gate)
    row_in(1, outer)
    send_down(1)
    steps = (z,) + far
    for i, at in enumerate(steps):
        up_in_y(i, at)
    own[0].wait()
    for i, at in enumerate(steps):
        arrive(up_at(1 - core, at * cols + y), base["up_c"] + i)
        arrive(up_at(1 - core, at * cols + 1 - y), base["up_c"] + lines + i)

    deep = sp * up.shape[2]

    def raise_rows(j):
        block_in = rows[j].reshape(lines * share, rows.shape[3])
        for origin in range(2):
            product = jnp.dot(
                block_in, up[origin].reshape(deep, width), preferred_element_type=f32
            )
            hidden_ref[
                j * lines * share : (j + 1) * lines * share, origin * width : (origin + 1) * width
            ] = jnp.square(jnp.maximum(product, 0.0)).astype(bf16)

    raise_rows(0)

    def down_in_z(upper):
        for i, at in enumerate(far):
            held = down_at(core, at * cols + y, upper)
            arrive(held, base["down_z"] + upper * lines + at)
            send(held, held, peer_y, base["down_y"] + upper * lines + 1 + i)
            send(held, held, peer_c, base["down_c"] + upper * 2 * lines + 1 + i)

    def down_in_y(upper):
        for i, at in enumerate(steps):
            held = down_at(core, at * cols + 1 - y, upper)
            arrive(held, base["down_y"] + upper * lines + i)
            send(held, held, peer_c, base["down_c"] + upper * 2 * lines + lines + i)

    units = (gate, outer, mate, z)

    def lower(chunk):
        upper, flipped = chunk // 2, chunk % 2
        column = (1 - y) if flipped else y
        for i, at in enumerate(steps):
            arrive(
                down_at(1 - core, at * cols + column, upper),
                base["down_c"] + upper * 2 * lines + flipped * lines + i,
            )
        total = None
        for origin in range(2):
            weight = down[origin, :, column, upper].reshape(lines * piece, width)
            product = lax.dot_general(
                hidden_ref[:, origin * width : (origin + 1) * width],
                weight,
                (((1,), (1,)), ((), ())),
                preferred_element_type=f32,
            )
            total = product if total is None else total + product
        part[chunk] = total[: lines * share].reshape(part.shape[1:])
        x_send[chunk] = total[lines * share :].astype(bf16).reshape(x_send.shape[1:])
        for i, at in enumerate(units):
            send(
                x_send.at[chunk, at],
                x_got.at[chunk, at],
                peer_x,
                base["sum_x"] + chunk * lines + i,
            )

    def pair(chunk, i):
        at = units[i]
        arrive(x_got.at[chunk, at], base["sum_x"] + chunk * lines + i)
        return part[chunk, at] + x_got[chunk, at].astype(f32)

    def gather_sums(chunk):
        far_sum = [
            pltpu.make_async_remote_copy(
                src_ref=z_send.at[chunk, i],
                dst_ref=r_got.at[chunk, i],
                send_sem=send_sem.at[len(started) + i],
                recv_sem=recv_sem.at[base["sum_r"] + chunk * 2 + i],
                device_id=line(mate),
                device_id_type=mesh_id,
            )
            for i in range(2)
        ]
        started.extend((edge, copy) for copy in far_sum)
        mate_sum = pltpu.make_async_remote_copy(
            src_ref=z_send.at[chunk, 2],
            dst_ref=m_got.at[chunk],
            send_sem=send_sem.at[len(started)],
            recv_sem=recv_sem.at[base["sum_m"] + chunk],
            device_id=line(mate),
            device_id_type=mesh_id,
        )
        started.append((None, mate_sum))
        across = [
            pltpu.make_async_remote_copy(
                src_ref=z_send.at[chunk, i],
                dst_ref=f_got.at[chunk],
                send_sem=send_sem.at[len(started) + i],
                recv_sem=recv_sem.at[base["sum_f"] + chunk],
                device_id=line(units[i]),
                device_id_type=mesh_id,
            )
            for i in range(2)
        ]
        started.extend((inner, copy) for copy in across)

        @pl.when(edge)
        def _():
            for i in range(2):
                z_send[chunk, i] = pair(chunk, i).astype(bf16)
                far_sum[i].start()
            z_send[chunk, 2] = pair(chunk, 2).astype(bf16)
            mate_sum.start()

        @pl.when(inner)
        def _():
            z_send[chunk, 2] = pair(chunk, 2).astype(bf16)
            mate_sum.start()
            for i in range(2):
                value = pair(chunk, i)
                arrive(r_got.at[chunk, i], base["sum_r"] + chunk * 2 + i)
                z_send[chunk, i] = (value + r_got[chunk, i].astype(f32)).astype(bf16)
                across[i].start()

    def finish(chunk):
        upper, flipped = chunk // 2, chunk % 2
        column = (1 - y) if flipped else y
        value = pair(chunk, 3)
        arrive(m_got.at[chunk], base["sum_m"] + chunk)
        value = value + m_got[chunk].astype(f32)
        arrive(f_got.at[chunk], base["sum_f"] + chunk)
        value = value + f_got[chunk].astype(f32)
        for i in range(lines):
            start = pl.multiple_of(((i * cols + column) * 2 + upper) * piece, piece)
            ffn_ref[:, pl.ds(start, piece)] = value[:, i * piece : (i + 1) * piece]

    down_in_z(0)
    for i, at in enumerate((z, gate, outer, mate)):
        arrive(rows.at[1, at], base["row_x"] + i)
    raise_rows(1)
    own[1].wait()
    own[2].wait()
    lower(0)
    down_in_y(0)
    lower(1)
    gather_sums(0)
    down_in_z(1)
    lower(2)
    gather_sums(1)
    down_in_y(1)
    lower(3)
    gather_sums(2)
    finish(0)
    finish(1)
    gather_sums(3)
    finish(2)
    finish(3)
    out_ref[...] = (mixed.astype(f32) + rms_scale(ffn_ref[...], last_ref[...])).astype(bf16)
    for cond, copy in started:
        if cond is None:
            copy.wait_send()
        else:
            pl.when(cond)(lambda: copy.wait_send())


def fast_local(
    resid,
    query_broad,
    query_narrow,
    latent,
    key_rope,
    latent_gain,
    key_up_broad,
    value_up_broad,
    key_up_narrow,
    value_up_narrow,
    out_broad,
    out_narrow,
    post_gain,
    ffn_gain,
    up_weight,
    down_weight,
    ffn_out_gain,
):
    sp = lax.axis_size("sp")
    tp = lax.axis_size("tp")
    cols = row_parts
    lines = sp // cols
    s = lax.axis_index("sp")
    z = s // cols
    y = s % cols
    local_rows = resid.shape[0]
    share_rows = local_rows // tp
    query_pos = s * local_rows + jnp.arange(local_rows, dtype=jnp.int32)
    rope_width = key_rope.shape[1]
    bf16 = jnp.bfloat16

    frequency = rope_base ** (-2.0 * jnp.arange(rope_width // 2, dtype=jnp.float32) / rope_width)
    angles = query_pos.astype(jnp.float32)[:, None] * frequency[None, :]
    cosine, sine = jnp.cos(angles), jnp.sin(angles)
    table = jnp.concatenate([cosine, cosine, -sine, sine], axis=1)
    half_rows = local_rows // 2
    both_width = latent.shape[1] + rope_width
    broad_width = key_up_broad.shape[1]
    narrow_width = key_up_narrow.shape[1]
    width = broad_width + narrow_width
    deep = resid.shape[1]
    slice_width = up_weight.shape[1] // lines
    vmem = pl.BlockSpec(memory_space=pltpu.VMEM)
    anywhere = pl.BlockSpec(memory_space=pl.ANY)
    chunks = 4
    heads = broad_width // DB + narrow_width // DN
    piece = up_weight.shape[0] // 2
    chunk_width = deep // chunks
    _, sems = sem_layout(lines, tp, chunks)
    f32 = jnp.float32
    return pl.pallas_call(
        functools.partial(layer_kernel, sp, tp),
        out_shape=jax.ShapeDtypeStruct((share_rows, deep), bf16),
        in_specs=[vmem] * 11 + [anywhere] * 2 + [vmem] * 3 + [anywhere] * 2,
        out_specs=vmem,
        scratch_shapes=[
            pltpu.VMEM((share_rows, both_width), bf16),
            pltpu.VMEM(query_broad.shape, bf16),
            pltpu.VMEM(query_narrow.shape, bf16),
            pltpu.VMEM((sp, tp, share_rows, both_width), bf16),
            pltpu.VMEM((heads, local_rows, 1), f32),
            pltpu.VMEM((heads, local_rows, 1), f32),
            pltpu.VMEM((heads, local_rows, lane_tile), f32),
            pltpu.VMEM((tp, share_rows, width), bf16),
            pltpu.VMEM((tp, share_rows, width), bf16),
            pltpu.VMEM(out_broad.shape, bf16),
            pltpu.VMEM(out_narrow.shape, bf16),
            pltpu.VMEM((2, sp, up_weight.shape[0], slice_width), bf16),
            pltpu.VMEM((2, lines, cols, 2, piece, slice_width), bf16),
            pltpu.VMEM((2, lines, share_rows, deep), bf16),
            pltpu.VMEM((2 * lines * share_rows, 2 * slice_width), bf16),
            pltpu.VMEM((chunks, lines, share_rows, chunk_width), f32),
            pltpu.VMEM((chunks, lines, share_rows, chunk_width), bf16),
            pltpu.VMEM((chunks, lines, share_rows, chunk_width), bf16),
            pltpu.VMEM((chunks, 3, share_rows, chunk_width), bf16),
            pltpu.VMEM((chunks, 2, share_rows, chunk_width), bf16),
            pltpu.VMEM((chunks, share_rows, chunk_width), bf16),
            pltpu.VMEM((chunks, share_rows, chunk_width), bf16),
            pltpu.VMEM((share_rows, deep), f32),
            pltpu.SemaphoreType.DMA((sems + lines * tp,)),
            pltpu.SemaphoreType.DMA((sems,)),
            pltpu.SemaphoreType.DMA((6,)),
        ],
        compiler_params=pltpu.CompilerParams(
            collective_id=0, has_side_effects=True, vmem_limit_bytes=60 * 2**20
        ),
    )(
        latent,
        key_rope,
        table,
        latent_gain[None],
        query_broad,
        query_narrow,
        resid,
        key_up_broad,
        value_up_broad,
        key_up_narrow,
        value_up_narrow,
        out_broad,
        out_narrow,
        post_gain[None],
        ffn_gain[None],
        ffn_out_gain[None],
        up_weight,
        down_weight,
    )


def solution(mesh):
    in_specs = (
        P("sp", None),
        P("sp", "tp"),
        P("sp", "tp"),
        P("sp", None),
        P("sp", None),
        P(),
        P(None, "tp"),
        P(None, "tp"),
        P(None, "tp"),
        P(None, "tp"),
        P(),
        P(),
        P(),
        P(),
        P("sp", "tp"),
        P("sp", "tp"),
        P(),
    )
    out_specs = P(("sp", "tp"), None)
    sp = mesh.shape["sp"]
    tp = mesh.shape["tp"]

    def whole(*args):
        hidden = args[14].shape[1] // tp
        rows = args[0].shape[0] // sp
        lines = sp // row_parts
        fits = (
            sp % row_parts == 0
            and tp & (tp - 1) == 0
            and tp == 4
            and lines == 4
            and hidden % (lines * lane_tile) == 0
            and args[0].shape[1] % (2 * lane_tile * sp) == 0
            and rows % (16 * tp) == 0
        )
        body = fast_local if fits else local
        return jax.shard_map(
            body, mesh=mesh, in_specs=in_specs, out_specs=out_specs, check_vma=False
        )(*args)

    return whole
```

```python
import functools
import math

import jax
import jax.numpy as jnp
from jax import lax
from jax.experimental import pallas as pl
from jax.experimental.pallas import tpu as pltpu
from jax.sharding import PartitionSpec as P

DB = 128
DN = 64


norm_eps = 1e-06
rope_base = 500000.0
masked_score = -1e30


def rotate(values, positions):
    full_width = values.shape[-1]
    half_width = full_width // 2
    frequency = rope_base ** (-2.0 * jnp.arange(half_width, dtype=jnp.float32) / full_width)
    angles = positions.astype(jnp.float32)[:, None] * frequency[None, :]
    angle_shape = (angles.shape[0],) + (1,) * (values.ndim - 2) + (half_width,)
    cosine = jnp.cos(angles).reshape(angle_shape)
    sine_part = jnp.sin(angles).reshape(angle_shape)
    leading = values[..., :half_width]
    trailing = values[..., half_width:]
    return jnp.concatenate(
        [leading * cosine - trailing * sine_part, trailing * cosine + leading * sine_part], axis=-1
    )


def rms_scale(values, norm_gain):
    return (
        values * lax.rsqrt(jnp.mean(values * values, axis=-1, keepdims=True) + norm_eps) * norm_gain
    )


def group_update(
    running, nope_query, rope_query, key_rows, key_rot, value_rows, score_scale, allowed
):
    old_max, old_sum, old_acc = running
    scores = jnp.einsum("qhd,khd->hqk", nope_query, key_rows, preferred_element_type=jnp.float32)
    scores = scores + jnp.einsum(
        "qhd,kd->hqk", rope_query, key_rot, preferred_element_type=jnp.float32
    )
    scores = jnp.where(allowed, scores * score_scale, masked_score)
    new_max = jnp.maximum(old_max, jnp.max(scores, axis=-1))
    exponent = jnp.where(allowed, jnp.exp(scores - new_max[:, :, None]), 0.0)
    factor = jnp.exp(old_max - new_max)
    new_sum = old_sum * factor + jnp.sum(exponent, axis=-1)
    weighted = jnp.einsum(
        "hqk,khd->qhd",
        exponent.astype(jnp.bfloat16),
        value_rows,
        preferred_element_type=jnp.float32,
    )
    new_acc = old_acc * jnp.transpose(factor)[:, :, None] + weighted
    return (new_max, new_sum, new_acc)


def local(
    resid,
    query_broad,
    query_narrow,
    latent,
    key_rope,
    latent_gain,
    key_up_broad,
    value_up_broad,
    key_up_narrow,
    value_up_narrow,
    out_broad,
    out_narrow,
    post_gain,
    ffn_gain,
    up_weight,
    down_weight,
    ffn_out_gain,
):
    local_rows = resid.shape[0]
    head_parts = lax.axis_size("tp")
    share_rows = local_rows // head_parts
    row_offset = lax.axis_index("sp") * local_rows
    last_query = row_offset + local_rows - 1
    query_pos = row_offset + jnp.arange(local_rows, dtype=jnp.int32)
    rope_width = key_rope.shape[1]
    broad_count = key_up_broad.shape[1] // DB
    narrow_count = key_up_narrow.shape[1] // DN
    broad_heads = query_broad.reshape(local_rows, broad_count, DB + rope_width)
    broad_nope = broad_heads[:, :, :DB]
    broad_rope = rotate(broad_heads[:, :, DB:].astype(jnp.float32), query_pos).astype(jnp.bfloat16)
    narrow_heads = query_narrow.reshape(local_rows, narrow_count, DN + rope_width)
    narrow_nope = narrow_heads[:, :, :DN]
    narrow_rope = rotate(narrow_heads[:, :, DN:].astype(jnp.float32), query_pos).astype(
        jnp.bfloat16
    )
    broad_scale = (DB + rope_width) ** (-0.5)
    narrow_scale = (DN + rope_width) ** (-0.5)

    def attend(running, latent_rows, rope_rows, first_row):
        key_count = latent_rows.shape[0]
        key_pos = first_row + jnp.arange(key_count, dtype=jnp.int32)
        latent_normed = rms_scale(latent_rows.astype(jnp.float32), latent_gain).astype(jnp.bfloat16)

        def expand(weight, head_size):
            product = jnp.dot(latent_normed, weight, preferred_element_type=jnp.float32)
            return product.astype(jnp.bfloat16).reshape(key_count, -1, head_size)

        key_rot = rotate(rope_rows.astype(jnp.float32), key_pos).astype(jnp.bfloat16)
        allowed = (key_pos[None, :] <= query_pos[:, None])[None]
        broad_state = group_update(
            running[0],
            broad_nope,
            broad_rope,
            expand(key_up_broad, DB),
            key_rot,
            expand(value_up_broad, DB),
            broad_scale,
            allowed,
        )
        narrow_state = group_update(
            running[1],
            narrow_nope,
            narrow_rope,
            expand(key_up_narrow, DN),
            key_rot,
            expand(value_up_narrow, DN),
            narrow_scale,
            allowed,
        )
        return (broad_state, narrow_state)

    def fresh(head_count, head_size):
        return (
            jnp.full((head_count, local_rows), masked_score, jnp.float32),
            jnp.zeros((head_count, local_rows), jnp.float32),
            jnp.zeros((local_rows, head_count, head_size), jnp.float32),
        )

    initial = (fresh(broad_count, DB), fresh(narrow_count, DN))
    latent_piece = lax.all_gather(latent, "sp", axis=0, tiled=True)
    rope_piece = lax.all_gather(key_rope, "sp", axis=0, tiled=True)
    piece_rows = latent_piece.shape[0]
    block_rows = math.gcd(piece_rows, 1024)

    def one_block(block_index, carried):
        begin = block_index * block_rows
        latent_block = lax.dynamic_slice_in_dim(latent_piece, begin, block_rows, 0)
        rope_block = lax.dynamic_slice_in_dim(rope_piece, begin, block_rows, 0)

        def unchanged(kept_state):
            return kept_state

        def updated(kept_state):
            return attend(kept_state, latent_block, rope_block, begin)

        return lax.cond(begin > last_query, unchanged, updated, carried)

    final_state = lax.fori_loop(0, piece_rows // block_rows, one_block, initial)

    def finish(running):
        run_max, run_sum, run_acc = running
        return (
            (run_acc / jnp.transpose(run_sum)[:, :, None])
            .astype(jnp.bfloat16)
            .reshape(local_rows, -1)
        )

    attn_broad = finish(final_state[0])
    attn_narrow = finish(final_state[1])
    rows_broad, rows_narrow = (
        lax.all_to_all(attn_broad, "tp", split_axis=0, concat_axis=1, tiled=True),
        lax.all_to_all(attn_narrow, "tp", split_axis=0, concat_axis=1, tiled=True),
    )
    projected = jnp.dot(rows_broad, out_broad, preferred_element_type=jnp.float32) + jnp.dot(
        rows_narrow, out_narrow, preferred_element_type=jnp.float32
    )
    own_resid = lax.dynamic_slice_in_dim(resid, lax.axis_index("tp") * share_rows, share_rows, 0)
    mixed = (own_resid.astype(jnp.float32) + rms_scale(projected, post_gain)).astype(jnp.bfloat16)
    normed = rms_scale(mixed.astype(jnp.float32), ffn_gain).astype(jnp.bfloat16)
    up_full, down_full = (
        lax.all_gather(up_weight, "sp", axis=0, tiled=True),
        lax.all_gather(down_weight, "sp", axis=0, tiled=True),
    )
    hidden = jnp.square(
        jax.nn.relu(
            jnp.dot(
                lax.all_gather(normed, "tp", axis=0, tiled=True),
                up_full,
                preferred_element_type=jnp.float32,
            )
        )
    ).astype(jnp.bfloat16)
    ffn = lax.psum_scatter(
        lax.dot_general(
            hidden, down_full, (((1,), (1,)), ((), ())), preferred_element_type=jnp.float32
        ).astype(jnp.bfloat16),
        "tp",
        scatter_dimension=0,
        tiled=True,
    ).astype(jnp.float32)
    return (mixed.astype(jnp.float32) + rms_scale(ffn, ffn_out_gain)).astype(jnp.bfloat16)

lane_tile = 128
row_parts = 2
mesh_id = pl.DeviceIdType.MESH


def sem_layout(lines, tp, chunks, row_chunks):
    sizes = {
        "lat_z": lines,
        "lat_y": lines,
        "lat_x": 2 * lines,
        "lat_c": 4 * lines,
        "up_z": lines,
        "up_y": lines,
        "up_c": 2 * lines,
        "down_z": 2 * lines,
        "down_y": 2 * lines,
        "down_c": 4 * lines,
        "heads": tp,
        "row_z": lines * row_chunks,
        "row_x": lines * row_chunks,
        "sum_x": chunks * lines,
        "sum_r": chunks * 2,
        "sum_m": chunks,
        "sum_f": chunks,
    }
    base, total = {}, 0
    for name, size in sizes.items():
        base[name] = total
        total += size
    return base, total


def layer_kernel(
    sp,
    tp,
    latent_ref,
    key_rope_ref,
    table_ref,
    latent_gain_ref,
    qb_in,
    qn_in,
    resid_ref,
    kb_ref,
    vb_ref,
    kn_ref,
    vn_ref,
    ob_hbm,
    on_hbm,
    post_ref,
    gain_ref,
    last_ref,
    up_hbm,
    down_hbm,
    out_ref,
    mine_ref,
    qb_ref,
    qn_ref,
    lat,
    top_ref,
    sum_ref,
    acc_ref,
    attn,
    heads,
    ob,
    on,
    up,
    down,
    rows,
    hidden_ref,
    part,
    x_send,
    x_got,
    z_send,
    r_got,
    m_got,
    f_got,
    ffn_ref,
    send_sem,
    recv_sem,
    local_sem,
    pair_sem,
):
    cols = row_parts
    lines = sp // cols
    groups = ((1, 2), (0, 3))
    chunks = len(groups)
    s = lax.axis_index("sp")
    t = lax.axis_index("tp")
    z = s // cols
    y = s % cols
    core = t % 2
    x = t // 2
    t_core = 2 * x + 1 - core
    t_x = 2 * (1 - x) + core
    t_both = 2 * (1 - x) + 1 - core
    s_y = z * cols + 1 - y
    half = z // 2
    mate = z + 1 - 2 * (z % 2)
    gate = 2 - half
    outer = 3 * (1 - half)
    inner = (z == 1) | (z == 2)
    edge = (z == 0) | (z == 3)
    bf16 = jnp.bfloat16
    f32 = jnp.float32
    share = resid_ref.shape[0] // tp
    block_rows = resid_ref.shape[0]
    width = up.shape[3]
    row_step = 16
    row_chunks = share // row_step
    base, _ = sem_layout(lines, tp, chunks, row_chunks)

    def line(at):
        return (at * cols + y, t)

    peer_y, peer_x, peer_c, peer_b = (s_y, t), (s, t_x), (s, t_core), (s, t_both)
    peers = [line(mate), line(gate), line(outer), peer_y, peer_x, peer_c, peer_b]
    barrier = pltpu.get_barrier_semaphore()
    for peer in peers:
        pl.semaphore_signal(barrier, inc=1, device_id=peer, device_id_type=mesh_id)

    rope = key_rope_ref.shape[1]
    half_rope = rope // 2

    def turn(values, table):
        values = values.astype(f32)
        swapped = jnp.concatenate([values[:, half_rope:], values[:, :half_rope]], axis=1)
        return (values * table[:, :rope] + swapped * table[:, rope:]).astype(bf16)

    latent_width = latent_ref.shape[1]
    mine_rows = pl.ds(pl.multiple_of(t * share, 16), share)
    mine_ref[:, :latent_width] = rms_scale(
        latent_ref[mine_rows, :].astype(f32), latent_gain_ref[...]
    ).astype(bf16)
    mine_ref[:, latent_width:] = turn(key_rope_ref[mine_rows, :], table_ref[mine_rows, :])
    pl.semaphore_wait(barrier, len(peers))

    started = []

    def send(src, dst, peer, recv, cond=None):
        copy = pltpu.make_async_remote_copy(
            src_ref=src,
            dst_ref=dst,
            send_sem=send_sem.at[len(started)],
            recv_sem=recv_sem.at[recv],
            device_id=peer,
            device_id_type=mesh_id,
        )
        started.append((cond, copy))
        if cond is None:
            copy.start()
        else:
            pl.when(cond)(lambda: copy.start())

    def arrive(dst, recv):
        pltpu.make_async_remote_copy(
            src_ref=dst,
            dst_ref=dst,
            send_sem=send_sem.at[0],
            recv_sem=recv_sem.at[recv],
            device_id=peer_c,
            device_id_type=mesh_id,
        ).wait_recv()

    locals_ = []

    def bring(src, dst):
        copy = pltpu.make_async_copy(src, dst, local_sem.at[len(locals_)])
        copy.start()
        locals_.append(copy)
        return copy

    def block(k, flipped):
        return (z - k) * cols + ((1 - y) if flipped else y)

    for k in range(lines - 1, 0, -1):
        send(mine_ref, lat.at[s, t], line(z + k), base["lat_z"] + k, z + k < lines)
    send(mine_ref, lat.at[s, t], peer_y, base["lat_y"])
    send(mine_ref, lat.at[s, t], peer_x, base["lat_x"])
    send(mine_ref, lat.at[s, t], peer_c, base["lat_c"])
    own_copy = bring(mine_ref, lat.at[s, t])

    def cut(ref, at):
        return ref.at[:, pl.ds(pl.multiple_of(at * width, width), width)]

    far = (gate, outer, mate)

    def up_at(origin, at):
        return up.at[origin, at]

    def down_at(origin, at, flipped=False):
        return down.at[origin, at, (1 - y) if flipped else y]

    def send_down(dest, cond=None):
        for i in range(2):
            send(
                down_half(cut(down_hbm, dest), i),
                down_half(down_at(core, z), i),
                line(dest),
                base["down_z"] + 2 * z + i,
                cond,
            )

    def down_half(ref, i):
        rows_half = down.shape[3] // 2
        return ref.at[pl.ds(i * rows_half, rows_half)]

    def send_up(dest, cond):
        send(cut(up_hbm, dest), up_at(core, s), line(dest), base["up_z"] + z, cond)

    send_up(mate, edge)
    for dest in far:
        send_up(dest, None if dest is not mate else inner)
    send_down(mate, inner)
    send_down(gate, z == 2)
    own = [bring(cut(up_hbm, z), up_at(core, s))]
    own.append(bring(cut(down_hbm, z), down_at(core, z)))
    outs = [bring(ob_hbm, ob), bring(on_hbm, on)]

    for queries, turned, size in ((qb_in, qb_ref, DB), (qn_in, qn_ref, DN)):
        step = size + rope
        for h in range(queries.shape[1] // step):
            middle = h * step + size
            turned[:, h * step : middle] = queries[:, h * step : middle]
            turned[:, middle : middle + rope] = turn(
                queries[:, middle : middle + rope], table_ref[...]
            )

    def when(k):
        return None if k == 0 else z >= k

    def guarded(k, body):
        if k == 0:
            body()
        else:
            pl.when(z >= k)(body)

    def lat_in_z(k):
        held = lat.at[block(k, False), t]
        guarded(k, lambda: arrive(held, base["lat_z"] + k))
        send(held, held, peer_y, base["lat_y"] + k, when(k))
        send(held, held, peer_x, base["lat_x"] + 2 * k, when(k))
        send(held, held, peer_c, base["lat_c"] + 4 * k, when(k))

    def lat_in_y(k):
        held = lat.at[block(k, True), t]
        guarded(k, lambda: arrive(held, base["lat_y"] + k))
        send(held, held, peer_x, base["lat_x"] + 2 * k + 1, when(k))
        send(held, held, peer_c, base["lat_c"] + 4 * k + 1, when(k))

    def lat_in_x(k):
        for i, flipped in enumerate((False, True)):
            held = lat.at[block(k, flipped), t_x]
            guarded(k, lambda: arrive(held, base["lat_x"] + 2 * k + i))
            send(held, held, peer_c, base["lat_c"] + 4 * k + 2 + i, when(k))

    broad = kb_ref.shape[1] // DB
    narrow = kn_ref.shape[1] // DN
    wb = DB + rope
    wn = DN + rope
    keys = cols * block_rows

    def attend(k):
        for i, flipped in enumerate((False, True)):
            arrive(lat.at[block(k, flipped), t_core], base["lat_c"] + 4 * k + i)
            arrive(lat.at[block(k, flipped), t_both], base["lat_c"] + 4 * k + 2 + i)
        both = lat[pl.ds((z - k) * cols, cols)].reshape(keys, latent_width + rope)
        normed = both[:, :latent_width]
        rot = both[:, latent_width:]

        def expand(ref):
            return jnp.dot(normed, ref[...], preferred_element_type=f32).astype(bf16)

        kb, vb, kn, vn = expand(kb_ref), expand(vb_ref), expand(kn_ref), expand(vn_ref)
        if k == 0:
            query_pos = y * block_rows + lax.broadcasted_iota(jnp.int32, (block_rows, keys), 0)
            allowed = lax.broadcasted_iota(jnp.int32, (block_rows, keys), 1) <= query_pos
        for h in range(broad + narrow):
            if h < broad:
                q = qb_ref[:, h * wb : (h + 1) * wb]
                key = jnp.concatenate([kb[:, h * DB : (h + 1) * DB], rot], axis=1)
                v = vb[:, h * DB : (h + 1) * DB]
                scale = wb ** (-0.5)
            else:
                n = h - broad
                q = qn_ref[:, n * wn : (n + 1) * wn]
                key = jnp.concatenate([kn[:, n * DN : (n + 1) * DN], rot], axis=1)
                v = vn
                scale = wn ** (-0.5)
            score = scale * lax.dot_general(
                q, key, (((1,), (1,)), ((), ())), preferred_element_type=f32
            )
            if k == 0:
                score = jnp.where(allowed, score, masked_score)
                new_max = jnp.max(score, axis=-1, keepdims=True)
                e = jnp.where(allowed, jnp.exp(score - new_max), 0.0)
                new_sum = jnp.sum(e, axis=-1, keepdims=True)
                acc_ref[h] = jnp.dot(e.astype(bf16), v, preferred_element_type=f32)
            else:
                old_max = top_ref[h]
                new_max = jnp.maximum(old_max, jnp.max(score, axis=-1, keepdims=True))
                e = jnp.exp(score - new_max)
                factor = jnp.exp(old_max - new_max)
                new_sum = sum_ref[h] * factor + jnp.sum(e, axis=-1, keepdims=True)
                acc_ref[h] = acc_ref[h] * factor + jnp.dot(
                    e.astype(bf16), v, preferred_element_type=f32
                )
            top_ref[h] = new_max
            sum_ref[h] = new_sum

    def up_in_z(i, at):
        held = up_at(core, at * cols + y)
        arrive(held, base["up_z"] + at)
        send(held, held, peer_y, base["up_y"] + 1 + i)
        send(held, held, peer_c, base["up_c"] + 1 + i)

    def down_in_z(at, cond=None):
        for i in range(2):
            held = down_half(down_at(core, at), i)
            if cond is None:
                arrive(held, base["down_z"] + 2 * at + i)
            else:
                pl.when(cond)(lambda: arrive(held, base["down_z"] + 2 * at + i))
            send(held, held, peer_y, base["down_y"] + 2 * at + i, cond)
            send(held, held, peer_c, base["down_c"] + 4 * at + i, cond)

    lat_in_y(0)
    lat_in_z(1)
    lat_in_z(2)
    lat_in_z(3)
    lat_in_x(0)
    send(cut(up_hbm, z), up_at(core, s), peer_y, base["up_y"])
    send(cut(up_hbm, z), up_at(core, s), peer_c, base["up_c"])
    own_copy.wait()
    attend(0)
    lat_in_y(1)
    lat_in_y(2)
    lat_in_y(3)
    lat_in_x(1)
    up_in_z(2, mate)
    for i in range(2):
        held = down_half(cut(down_hbm, z), i)
        own_half = down_half(down_at(core, z), i)
        send(held, own_half, peer_y, base["down_y"] + 2 * z + i)
        send(held, own_half, peer_c, base["down_c"] + 4 * z + i)
    guarded(1, lambda: attend(1))
    lat_in_x(2)
    lat_in_x(3)
    guarded(2, lambda: attend(2))
    guarded(3, lambda: attend(3))

    parts = [acc_ref[h] / sum_ref[h] for h in range(broad + narrow)]
    for h in range(broad):
        for i in range(tp):
            attn[i, :, h * DB : (h + 1) * DB] = parts[h][i * share : (i + 1) * share].astype(bf16)
    column = lax.broadcasted_iota(jnp.int32, parts[broad].shape, 1)
    merged = parts[broad]
    for n in range(1, narrow):
        merged = jnp.where(column >= n * DN, parts[broad + n], merged)
    for i in range(tp):
        attn[i, :, broad * DB :] = merged[i * share : (i + 1) * share].astype(bf16)

    turned_to = ((t_x, peer_x), (t_both, peer_b), (t_core, peer_c))
    for i, (at, peer) in enumerate(turned_to):
        send(attn.at[at], heads.at[t], peer, base["heads"] + i)
    heads[t] = attn[t]
    for copy in outs:
        copy.wait()
    for i, (at, _) in enumerate(turned_to):
        arrive(heads.at[at], base["heads"] + i)

    down_in_z(mate, edge)
    broad_width = kb_ref.shape[1]
    narrow_width = kn_ref.shape[1]
    projected = jnp.zeros((share, ob.shape[1]), f32)
    for i in range(tp):
        projected = projected + jnp.dot(
            heads[i, :, :broad_width],
            ob[i * broad_width : (i + 1) * broad_width],
            preferred_element_type=f32,
        )
        projected = projected + jnp.dot(
            heads[i, :, broad_width:],
            on[i * narrow_width : (i + 1) * narrow_width],
            preferred_element_type=f32,
        )
    mixed = (
        resid_ref[pl.ds(pl.multiple_of(t * share, 16), share), :].astype(f32)
        + rms_scale(projected, post_ref[...])
    ).astype(bf16)
    rows[0, z] = rms_scale(mixed.astype(f32), gain_ref[...]).astype(bf16)

    def row_piece(side, at, c):
        return rows.at[side, at, pl.ds(c * row_step, row_step)]

    crossing = []
    for dest in (gate, mate):
        for c in range(row_chunks):
            held = row_piece(0, z, c)
            send(held, held, line(dest), base["row_z"] + z * row_chunks + c)
            if dest is gate:
                crossing.append(started.pop()[1])
                started.append((edge, crossing[-1]))
                send(held, row_piece(1, z, c), peer_x, base["row_x"] + c)
    send_down(mate, edge)
    send_down(gate, z == 3)

    def up_in_y(i, at):
        held = up_at(core, at * cols + 1 - y)
        arrive(held, base["up_y"] + i)
        send(held, held, peer_c, base["up_c"] + lines + i)

    def row_in(i, at):
        for c in range(row_chunks):
            held = row_piece(0, at, c)
            index = base["row_z"] + at * row_chunks + c
            arrive(held, index)
            if i < 2:
                send(held, held, line(mate), index, inner)
            send(held, row_piece(1, at, c), peer_x, base["row_x"] + (1 + i) * row_chunks + c)

    up_in_z(0, gate)
    up_in_z(1, outer)
    row_in(2, mate)
    row_in(0, gate)
    row_in(1, outer)
    @pl.when(inner)
    def _():
        for copy in crossing:
            copy.wait_send()
        pl.semaphore_signal(pair_sem, inc=1, device_id=peer_c, device_id_type=mesh_id)
        pl.semaphore_wait(pair_sem, 1)

    send_down(gate, z == 1)
    send_down(outer, inner)
    steps = (z,) + far
    down_in_z(mate, inner)
    for i, at in enumerate(steps):
        up_in_y(i, at)
    own[0].wait()
    for i, at in enumerate(steps):
        arrive(up_at(1 - core, at * cols + y), base["up_c"] + i)
        arrive(up_at(1 - core, at * cols + 1 - y), base["up_c"] + lines + i)

    deep = sp * up.shape[2]

    def raise_rows(j):
        block_in = rows[j].reshape(lines * share, rows.shape[3])
        for origin in range(2):
            product = jnp.dot(
                block_in, up[origin].reshape(deep, width), preferred_element_type=f32
            )
            hidden_ref[
                j * lines * share : (j + 1) * lines * share, origin * width : (origin + 1) * width
            ] = jnp.square(jnp.maximum(product, 0.0)).astype(bf16)

    raise_rows(0)
    send_down(gate, z == 0)
    send_down(outer, edge)

    def down_in_y(at):
        for i in range(2):
            held = down_half(down_at(core, at, True), i)
            arrive(held, base["down_y"] + 2 * at + i)
            send(held, held, peer_c, base["down_c"] + 4 * at + 2 + i)

    units = (gate, outer, mate, z)

    span = part.shape[3] // 2

    def lower(group):
        for j, at in enumerate(groups[group]):
            for k, flipped in enumerate((False, True)):
                for i in range(2):
                    held = down_half(down_at(1 - core, at, flipped), i)
                    arrive(held, base["down_c"] + 4 * at + 2 * k + i)
            total = None
            for origin in range(2):
                product = lax.dot_general(
                    hidden_ref[:, origin * width : (origin + 1) * width],
                    down[origin, at].reshape(span, width),
                    (((1,), (1,)), ((), ())),
                    preferred_element_type=f32,
                )
                total = product if total is None else total + product
            total = total.reshape(2, lines, share, span)
            part[group, :, :, j * span : (j + 1) * span] = total[0]
            x_send[group, :, :, j * span : (j + 1) * span] = total[1].astype(bf16)
        for i, at in enumerate(units):
            send(
                x_send.at[group, at],
                x_got.at[group, at],
                peer_x,
                base["sum_x"] + group * lines + i,
            )

    def pair(chunk, i):
        at = units[i]
        arrive(x_got.at[chunk, at], base["sum_x"] + chunk * lines + i)
        return part[chunk, at] + x_got[chunk, at].astype(f32)

    def gather_sums(chunk):
        far_sum = [
            pltpu.make_async_remote_copy(
                src_ref=z_send.at[chunk, i],
                dst_ref=r_got.at[chunk, i],
                send_sem=send_sem.at[len(started) + i],
                recv_sem=recv_sem.at[base["sum_r"] + chunk * 2 + i],
                device_id=line(mate),
                device_id_type=mesh_id,
            )
            for i in range(2)
        ]
        started.extend((edge, copy) for copy in far_sum)
        mate_sum = pltpu.make_async_remote_copy(
            src_ref=z_send.at[chunk, 2],
            dst_ref=m_got.at[chunk],
            send_sem=send_sem.at[len(started)],
            recv_sem=recv_sem.at[base["sum_m"] + chunk],
            device_id=line(mate),
            device_id_type=mesh_id,
        )
        started.append((None, mate_sum))
        across = [
            pltpu.make_async_remote_copy(
                src_ref=z_send.at[chunk, i],
                dst_ref=f_got.at[chunk],
                send_sem=send_sem.at[len(started) + i],
                recv_sem=recv_sem.at[base["sum_f"] + chunk],
                device_id=line(units[i]),
                device_id_type=mesh_id,
            )
            for i in range(2)
        ]
        started.extend((inner, copy) for copy in across)

        def edge_part():
            for i in range(2):
                z_send[chunk, i] = pair(chunk, i).astype(bf16)
                far_sum[i].start()
            z_send[chunk, 2] = pair(chunk, 2).astype(bf16)
            mate_sum.start()

        def inner_part():
            z_send[chunk, 2] = pair(chunk, 2).astype(bf16)
            mate_sum.start()
            for i in range(2):
                value = pair(chunk, i)
                arrive(r_got.at[chunk, i], base["sum_r"] + chunk * 2 + i)
                z_send[chunk, i] = (value + r_got[chunk, i].astype(f32)).astype(bf16)
                across[i].start()

        pl.when(edge)(edge_part)
        pl.when(inner)(inner_part)

    def finish(chunk):
        value = pair(chunk, 3)
        arrive(m_got.at[chunk], base["sum_m"] + chunk)
        value = value + m_got[chunk].astype(f32)
        arrive(f_got.at[chunk], base["sum_f"] + chunk)
        value = value + f_got[chunk].astype(f32)
        for j, at in enumerate(groups[chunk]):
            ffn_ref[:, at * span : (at + 1) * span] = value[:, j * span : (j + 1) * span]

    for i, at in enumerate((z, gate, outer, mate)):
        for c in range(row_chunks):
            arrive(row_piece(1, at, c), base["row_x"] + i * row_chunks + c)
    raise_rows(1)
    own[1].wait()
    down_in_z(gate)
    down_in_y(1)
    down_in_y(2)
    lower(0)
    down_in_z(outer)
    down_in_y(0)
    down_in_y(3)
    lower(1)
    gather_sums(0)
    gather_sums(1)
    finish(0)
    finish(1)
    out_ref[...] = (mixed.astype(f32) + rms_scale(ffn_ref[...], last_ref[...])).astype(bf16)
    for cond, copy in started:
        if cond is None:
            copy.wait_send()
        else:
            pl.when(cond)(lambda: copy.wait_send())


def fast_local(
    resid,
    query_broad,
    query_narrow,
    latent,
    key_rope,
    latent_gain,
    key_up_broad,
    value_up_broad,
    key_up_narrow,
    value_up_narrow,
    out_broad,
    out_narrow,
    post_gain,
    ffn_gain,
    up_weight,
    down_weight,
    ffn_out_gain,
):
    sp = lax.axis_size("sp")
    tp = lax.axis_size("tp")
    cols = row_parts
    lines = sp // cols
    s = lax.axis_index("sp")
    z = s // cols
    y = s % cols
    local_rows = resid.shape[0]
    share_rows = local_rows // tp
    query_pos = s * local_rows + jnp.arange(local_rows, dtype=jnp.int32)
    rope_width = key_rope.shape[1]
    bf16 = jnp.bfloat16

    frequency = rope_base ** (-2.0 * jnp.arange(rope_width // 2, dtype=jnp.float32) / rope_width)
    angles = query_pos.astype(jnp.float32)[:, None] * frequency[None, :]
    cosine, sine = jnp.cos(angles), jnp.sin(angles)
    table = jnp.concatenate([cosine, cosine, -sine, sine], axis=1)
    half_rows = local_rows // 2
    both_width = latent.shape[1] + rope_width
    broad_width = key_up_broad.shape[1]
    narrow_width = key_up_narrow.shape[1]
    width = broad_width + narrow_width
    deep = resid.shape[1]
    slice_width = up_weight.shape[1] // lines
    vmem = pl.BlockSpec(memory_space=pltpu.VMEM)
    anywhere = pl.BlockSpec(memory_space=pl.ANY)
    chunks = 2
    heads = broad_width // DB + narrow_width // DN
    chunk_width = deep // chunks
    _, sems = sem_layout(lines, tp, chunks, share_rows // 16)
    f32 = jnp.float32
    return pl.pallas_call(
        functools.partial(layer_kernel, sp, tp),
        out_shape=jax.ShapeDtypeStruct((share_rows, deep), bf16),
        in_specs=[vmem] * 11 + [anywhere] * 2 + [vmem] * 3 + [anywhere] * 2,
        out_specs=vmem,
        scratch_shapes=[
            pltpu.VMEM((share_rows, both_width), bf16),
            pltpu.VMEM(query_broad.shape, bf16),
            pltpu.VMEM(query_narrow.shape, bf16),
            pltpu.VMEM((sp, tp, share_rows, both_width), bf16),
            pltpu.VMEM((heads, local_rows, 1), f32),
            pltpu.VMEM((heads, local_rows, 1), f32),
            pltpu.VMEM((heads, local_rows, lane_tile), f32),
            pltpu.VMEM((tp, share_rows, width), bf16),
            pltpu.VMEM((tp, share_rows, width), bf16),
            pltpu.VMEM(out_broad.shape, bf16),
            pltpu.VMEM(out_narrow.shape, bf16),
            pltpu.VMEM((2, sp, up_weight.shape[0], slice_width), bf16),
            pltpu.VMEM((2, lines, cols, down_weight.shape[0], slice_width), bf16),
            pltpu.VMEM((2, lines, share_rows, deep), bf16),
            pltpu.VMEM((2 * lines * share_rows, 2 * slice_width), bf16),
            pltpu.VMEM((chunks, lines, share_rows, chunk_width), f32),
            pltpu.VMEM((chunks, lines, share_rows, chunk_width), bf16),
            pltpu.VMEM((chunks, lines, share_rows, chunk_width), bf16),
            pltpu.VMEM((chunks, 3, share_rows, chunk_width), bf16),
            pltpu.VMEM((chunks, 2, share_rows, chunk_width), bf16),
            pltpu.VMEM((chunks, share_rows, chunk_width), bf16),
            pltpu.VMEM((chunks, share_rows, chunk_width), bf16),
            pltpu.VMEM((share_rows, deep), f32),
            pltpu.SemaphoreType.DMA((2 * sems,)),
            pltpu.SemaphoreType.DMA((sems,)),
            pltpu.SemaphoreType.DMA((5,)),
            pltpu.SemaphoreType.REGULAR,
        ],
        compiler_params=pltpu.CompilerParams(
            collective_id=0, has_side_effects=True, vmem_limit_bytes=60 * 2**20
        ),
    )(
        latent,
        key_rope,
        table,
        latent_gain[None],
        query_broad,
        query_narrow,
        resid,
        key_up_broad,
        value_up_broad,
        key_up_narrow,
        value_up_narrow,
        out_broad,
        out_narrow,
        post_gain[None],
        ffn_gain[None],
        ffn_out_gain[None],
        up_weight,
        down_weight,
    )


def solution(mesh):
    in_specs = (
        P("sp", None),
        P("sp", "tp"),
        P("sp", "tp"),
        P("sp", None),
        P("sp", None),
        P(),
        P(None, "tp"),
        P(None, "tp"),
        P(None, "tp"),
        P(None, "tp"),
        P(),
        P(),
        P(),
        P(),
        P("sp", "tp"),
        P("sp", "tp"),
        P(),
    )
    out_specs = P(("sp", "tp"), None)
    sp = mesh.shape["sp"]
    tp = mesh.shape["tp"]

    def whole(*args):
        hidden = args[14].shape[1] // tp
        rows = args[0].shape[0] // sp
        lines = sp // row_parts
        fits = (
            sp % row_parts == 0
            and tp & (tp - 1) == 0
            and tp == 4
            and lines == 4
            and hidden % (lines * lane_tile) == 0
            and args[0].shape[1] % (2 * lane_tile * sp) == 0
            and rows % (16 * tp) == 0
        )
        body = fast_local if fits else local
        return jax.shard_map(
            body, mesh=mesh, in_specs=in_specs, out_specs=out_specs, check_vma=False
        )(*args)

    return whole
```

```python
import functools
import math

import jax
import jax.numpy as jnp
from jax import lax
from jax.experimental import pallas as pl
from jax.experimental.pallas import tpu as pltpu
from jax.sharding import PartitionSpec as P

DB = 128
DN = 64


norm_eps = 1e-06
rope_base = 500000.0
masked_score = -1e30


def rotate(values, positions):
    full_width = values.shape[-1]
    half_width = full_width // 2
    frequency = rope_base ** (-2.0 * jnp.arange(half_width, dtype=jnp.float32) / full_width)
    angles = positions.astype(jnp.float32)[:, None] * frequency[None, :]
    angle_shape = (angles.shape[0],) + (1,) * (values.ndim - 2) + (half_width,)
    cosine = jnp.cos(angles).reshape(angle_shape)
    sine_part = jnp.sin(angles).reshape(angle_shape)
    leading = values[..., :half_width]
    trailing = values[..., half_width:]
    return jnp.concatenate(
        [leading * cosine - trailing * sine_part, trailing * cosine + leading * sine_part], axis=-1
    )


def rms_scale(values, norm_gain):
    return (
        values * lax.rsqrt(jnp.mean(values * values, axis=-1, keepdims=True) + norm_eps) * norm_gain
    )


def group_update(
    running, nope_query, rope_query, key_rows, key_rot, value_rows, score_scale, allowed
):
    old_max, old_sum, old_acc = running
    scores = jnp.einsum("qhd,khd->hqk", nope_query, key_rows, preferred_element_type=jnp.float32)
    scores = scores + jnp.einsum(
        "qhd,kd->hqk", rope_query, key_rot, preferred_element_type=jnp.float32
    )
    scores = jnp.where(allowed, scores * score_scale, masked_score)
    new_max = jnp.maximum(old_max, jnp.max(scores, axis=-1))
    exponent = jnp.where(allowed, jnp.exp(scores - new_max[:, :, None]), 0.0)
    factor = jnp.exp(old_max - new_max)
    new_sum = old_sum * factor + jnp.sum(exponent, axis=-1)
    weighted = jnp.einsum(
        "hqk,khd->qhd",
        exponent.astype(jnp.bfloat16),
        value_rows,
        preferred_element_type=jnp.float32,
    )
    new_acc = old_acc * jnp.transpose(factor)[:, :, None] + weighted
    return (new_max, new_sum, new_acc)


def local(
    resid,
    query_broad,
    query_narrow,
    latent,
    key_rope,
    latent_gain,
    key_up_broad,
    value_up_broad,
    key_up_narrow,
    value_up_narrow,
    out_broad,
    out_narrow,
    post_gain,
    ffn_gain,
    up_weight,
    down_weight,
    ffn_out_gain,
):
    local_rows = resid.shape[0]
    head_parts = lax.axis_size("tp")
    share_rows = local_rows // head_parts
    row_offset = lax.axis_index("sp") * local_rows
    last_query = row_offset + local_rows - 1
    query_pos = row_offset + jnp.arange(local_rows, dtype=jnp.int32)
    rope_width = key_rope.shape[1]
    broad_count = key_up_broad.shape[1] // DB
    narrow_count = key_up_narrow.shape[1] // DN
    broad_heads = query_broad.reshape(local_rows, broad_count, DB + rope_width)
    broad_nope = broad_heads[:, :, :DB]
    broad_rope = rotate(broad_heads[:, :, DB:].astype(jnp.float32), query_pos).astype(jnp.bfloat16)
    narrow_heads = query_narrow.reshape(local_rows, narrow_count, DN + rope_width)
    narrow_nope = narrow_heads[:, :, :DN]
    narrow_rope = rotate(narrow_heads[:, :, DN:].astype(jnp.float32), query_pos).astype(
        jnp.bfloat16
    )
    broad_scale = (DB + rope_width) ** (-0.5)
    narrow_scale = (DN + rope_width) ** (-0.5)

    def attend(running, latent_rows, rope_rows, first_row):
        key_count = latent_rows.shape[0]
        key_pos = first_row + jnp.arange(key_count, dtype=jnp.int32)
        latent_normed = rms_scale(latent_rows.astype(jnp.float32), latent_gain).astype(jnp.bfloat16)

        def expand(weight, head_size):
            product = jnp.dot(latent_normed, weight, preferred_element_type=jnp.float32)
            return product.astype(jnp.bfloat16).reshape(key_count, -1, head_size)

        key_rot = rotate(rope_rows.astype(jnp.float32), key_pos).astype(jnp.bfloat16)
        allowed = (key_pos[None, :] <= query_pos[:, None])[None]
        broad_state = group_update(
            running[0],
            broad_nope,
            broad_rope,
            expand(key_up_broad, DB),
            key_rot,
            expand(value_up_broad, DB),
            broad_scale,
            allowed,
        )
        narrow_state = group_update(
            running[1],
            narrow_nope,
            narrow_rope,
            expand(key_up_narrow, DN),
            key_rot,
            expand(value_up_narrow, DN),
            narrow_scale,
            allowed,
        )
        return (broad_state, narrow_state)

    def fresh(head_count, head_size):
        return (
            jnp.full((head_count, local_rows), masked_score, jnp.float32),
            jnp.zeros((head_count, local_rows), jnp.float32),
            jnp.zeros((local_rows, head_count, head_size), jnp.float32),
        )

    initial = (fresh(broad_count, DB), fresh(narrow_count, DN))
    latent_piece = lax.all_gather(latent, "sp", axis=0, tiled=True)
    rope_piece = lax.all_gather(key_rope, "sp", axis=0, tiled=True)
    piece_rows = latent_piece.shape[0]
    block_rows = math.gcd(piece_rows, 1024)

    def one_block(block_index, carried):
        begin = block_index * block_rows
        latent_block = lax.dynamic_slice_in_dim(latent_piece, begin, block_rows, 0)
        rope_block = lax.dynamic_slice_in_dim(rope_piece, begin, block_rows, 0)

        def unchanged(kept_state):
            return kept_state

        def updated(kept_state):
            return attend(kept_state, latent_block, rope_block, begin)

        return lax.cond(begin > last_query, unchanged, updated, carried)

    final_state = lax.fori_loop(0, piece_rows // block_rows, one_block, initial)

    def finish(running):
        run_max, run_sum, run_acc = running
        return (
            (run_acc / jnp.transpose(run_sum)[:, :, None])
            .astype(jnp.bfloat16)
            .reshape(local_rows, -1)
        )

    attn_broad = finish(final_state[0])
    attn_narrow = finish(final_state[1])
    rows_broad, rows_narrow = (
        lax.all_to_all(attn_broad, "tp", split_axis=0, concat_axis=1, tiled=True),
        lax.all_to_all(attn_narrow, "tp", split_axis=0, concat_axis=1, tiled=True),
    )
    projected = jnp.dot(rows_broad, out_broad, preferred_element_type=jnp.float32) + jnp.dot(
        rows_narrow, out_narrow, preferred_element_type=jnp.float32
    )
    own_resid = lax.dynamic_slice_in_dim(resid, lax.axis_index("tp") * share_rows, share_rows, 0)
    mixed = (own_resid.astype(jnp.float32) + rms_scale(projected, post_gain)).astype(jnp.bfloat16)
    normed = rms_scale(mixed.astype(jnp.float32), ffn_gain).astype(jnp.bfloat16)
    up_full, down_full = (
        lax.all_gather(up_weight, "sp", axis=0, tiled=True),
        lax.all_gather(down_weight, "sp", axis=0, tiled=True),
    )
    hidden = jnp.square(
        jax.nn.relu(
            jnp.dot(
                lax.all_gather(normed, "tp", axis=0, tiled=True),
                up_full,
                preferred_element_type=jnp.float32,
            )
        )
    ).astype(jnp.bfloat16)
    ffn = lax.psum_scatter(
        lax.dot_general(
            hidden, down_full, (((1,), (1,)), ((), ())), preferred_element_type=jnp.float32
        ).astype(jnp.bfloat16),
        "tp",
        scatter_dimension=0,
        tiled=True,
    ).astype(jnp.float32)
    return (mixed.astype(jnp.float32) + rms_scale(ffn, ffn_out_gain)).astype(jnp.bfloat16)

lane_tile = 128
row_parts = 2
mesh_id = pl.DeviceIdType.MESH


def sem_layout(lines, tp, chunks, row_chunks):
    sizes = {
        "lat_z": lines,
        "lat_y": lines,
        "lat_x": 2 * lines,
        "lat_c": 4 * lines,
        "up_z": lines,
        "up_y": lines,
        "up_c": 2 * lines,
        "down_z": 2 * lines,
        "down_y": 2 * lines,
        "down_c": 4 * lines,
        "heads": tp,
        "row_z": lines * row_chunks,
        "row_x": lines * row_chunks,
        "sum_x": chunks * lines,
        "sum_r": chunks * 2,
        "sum_m": chunks,
        "sum_f": chunks,
    }
    base, total = {}, 0
    for name, size in sizes.items():
        base[name] = total
        total += size
    return base, total


def layer_kernel(
    sp,
    tp,
    latent_ref,
    key_rope_ref,
    table_ref,
    latent_gain_ref,
    qb_in,
    qn_in,
    resid_ref,
    kb_ref,
    vb_ref,
    kn_ref,
    vn_ref,
    ob_hbm,
    on_hbm,
    post_ref,
    gain_ref,
    last_ref,
    up_hbm,
    down_hbm,
    out_ref,
    mine_ref,
    qb_ref,
    qn_ref,
    lat,
    top_ref,
    sum_ref,
    acc_ref,
    attn,
    heads,
    ob,
    on,
    up,
    down,
    rows,
    hidden_ref,
    part,
    x_send,
    x_got,
    z_send,
    r_got,
    m_got,
    f_got,
    ffn_ref,
    send_sem,
    recv_sem,
    local_sem,
    pair_sem,
):
    cols = row_parts
    lines = sp // cols
    chunks = 5
    s = lax.axis_index("sp")
    t = lax.axis_index("tp")
    z = s // cols
    y = s % cols
    core = t % 2
    x = t // 2
    t_core = 2 * x + 1 - core
    t_x = 2 * (1 - x) + core
    t_both = 2 * (1 - x) + 1 - core
    s_y = z * cols + 1 - y
    half = z // 2
    mate = z + 1 - 2 * (z % 2)
    gate = 2 - half
    outer = 3 * (1 - half)
    inner = (z == 1) | (z == 2)
    edge = (z == 0) | (z == 3)
    bf16 = jnp.bfloat16
    f32 = jnp.float32
    share = resid_ref.shape[0] // tp
    block_rows = resid_ref.shape[0]
    width = up.shape[3]
    row_step = 16
    row_chunks = share // row_step
    base, _ = sem_layout(lines, tp, chunks, row_chunks)

    def line(at):
        return (at * cols + y, t)

    peer_y, peer_x, peer_c, peer_b = (s_y, t), (s, t_x), (s, t_core), (s, t_both)
    peers = [line(mate), line(gate), line(outer), peer_y, peer_x, peer_c, peer_b]
    barrier = pltpu.get_barrier_semaphore()
    for peer in peers:
        pl.semaphore_signal(barrier, inc=1, device_id=peer, device_id_type=mesh_id)

    rope = key_rope_ref.shape[1]
    half_rope = rope // 2

    def turn(values, table):
        values = values.astype(f32)
        swapped = jnp.concatenate([values[:, half_rope:], values[:, :half_rope]], axis=1)
        return (values * table[:, :rope] + swapped * table[:, rope:]).astype(bf16)

    latent_width = latent_ref.shape[1]
    mine_rows = pl.ds(pl.multiple_of(t * share, 16), share)
    mine_ref[:, :latent_width] = rms_scale(
        latent_ref[mine_rows, :].astype(f32), latent_gain_ref[...]
    ).astype(bf16)
    mine_ref[:, latent_width:] = turn(key_rope_ref[mine_rows, :], table_ref[mine_rows, :])
    pl.semaphore_wait(barrier, len(peers))

    started = []

    def send(src, dst, peer, recv, cond=None):
        copy = pltpu.make_async_remote_copy(
            src_ref=src,
            dst_ref=dst,
            send_sem=send_sem.at[len(started)],
            recv_sem=recv_sem.at[recv],
            device_id=peer,
            device_id_type=mesh_id,
        )
        started.append((cond, copy))
        if cond is None:
            copy.start()
        else:
            pl.when(cond)(lambda: copy.start())

    def arrive(dst, recv):
        pltpu.make_async_remote_copy(
            src_ref=dst,
            dst_ref=dst,
            send_sem=send_sem.at[0],
            recv_sem=recv_sem.at[recv],
            device_id=peer_c,
            device_id_type=mesh_id,
        ).wait_recv()

    locals_ = []

    def bring(src, dst):
        copy = pltpu.make_async_copy(src, dst, local_sem.at[len(locals_)])
        copy.start()
        locals_.append(copy)
        return copy

    def block(k, flipped):
        return (z - k) * cols + ((1 - y) if flipped else y)

    for k in range(lines - 1, 0, -1):
        send(mine_ref, lat.at[s, t], line(z + k), base["lat_z"] + k, z + k < lines)
    send(mine_ref, lat.at[s, t], peer_y, base["lat_y"])
    send(mine_ref, lat.at[s, t], peer_x, base["lat_x"])
    send(mine_ref, lat.at[s, t], peer_c, base["lat_c"])
    own_copy = bring(mine_ref, lat.at[s, t])

    def cut(ref, at):
        return ref.at[:, pl.ds(pl.multiple_of(at * width, width), width)]

    far = (gate, outer, mate)

    def up_at(origin, at):
        return up.at[origin, at]

    def down_at(origin, at, flipped=False):
        return down.at[origin, at, (1 - y) if flipped else y]

    def send_down(dest, cond=None):
        for i in range(2):
            send(
                down_half(cut(down_hbm, dest), i),
                down_half(down_at(core, z), i),
                line(dest),
                base["down_z"] + 2 * z + i,
                cond,
            )

    def down_half(ref, i):
        rows_half = down.shape[3] // 2
        return ref.at[pl.ds(i * rows_half, rows_half)]

    def send_up(dest, cond):
        send(cut(up_hbm, dest), up_at(core, s), line(dest), base["up_z"] + z, cond)

    send_up(mate, edge)
    for dest in far:
        send_up(dest, None if dest is not mate else inner)
    send_down(mate, inner)
    send_down(gate, z == 2)
    own = [bring(cut(up_hbm, z), up_at(core, s))]
    own.append(bring(cut(down_hbm, z), down_at(core, z)))
    outs = [bring(ob_hbm, ob), bring(on_hbm, on)]

    for queries, turned, size in ((qb_in, qb_ref, DB), (qn_in, qn_ref, DN)):
        step = size + rope
        for h in range(queries.shape[1] // step):
            middle = h * step + size
            turned[:, h * step : middle] = queries[:, h * step : middle]
            turned[:, middle : middle + rope] = turn(
                queries[:, middle : middle + rope], table_ref[...]
            )

    def when(k):
        return None if k == 0 else z >= k

    def guarded(k, body):
        if k == 0:
            body()
        else:
            pl.when(z >= k)(body)

    def lat_in_z(k):
        held = lat.at[block(k, False), t]
        guarded(k, lambda: arrive(held, base["lat_z"] + k))
        send(held, held, peer_y, base["lat_y"] + k, when(k))
        send(held, held, peer_x, base["lat_x"] + 2 * k, when(k))
        send(held, held, peer_c, base["lat_c"] + 4 * k, when(k))

    def lat_in_y(k):
        held = lat.at[block(k, True), t]
        guarded(k, lambda: arrive(held, base["lat_y"] + k))
        send(held, held, peer_x, base["lat_x"] + 2 * k + 1, when(k))
        send(held, held, peer_c, base["lat_c"] + 4 * k + 1, when(k))

    def lat_in_x(k):
        for i, flipped in enumerate((False, True)):
            held = lat.at[block(k, flipped), t_x]
            guarded(k, lambda: arrive(held, base["lat_x"] + 2 * k + i))
            send(held, held, peer_c, base["lat_c"] + 4 * k + 2 + i, when(k))

    broad = kb_ref.shape[1] // DB
    narrow = kn_ref.shape[1] // DN
    wb = DB + rope
    wn = DN + rope
    keys = cols * block_rows

    def attend(k):
        for i, flipped in enumerate((False, True)):
            arrive(lat.at[block(k, flipped), t_core], base["lat_c"] + 4 * k + i)
            arrive(lat.at[block(k, flipped), t_both], base["lat_c"] + 4 * k + 2 + i)
        both = lat[pl.ds((z - k) * cols, cols)].reshape(keys, latent_width + rope)
        normed = both[:, :latent_width]
        rot = both[:, latent_width:]

        def expand(ref):
            return jnp.dot(normed, ref[...], preferred_element_type=f32).astype(bf16)

        kb, vb, kn, vn = expand(kb_ref), expand(vb_ref), expand(kn_ref), expand(vn_ref)
        if k == 0:
            query_pos = y * block_rows + lax.broadcasted_iota(jnp.int32, (block_rows, keys), 0)
            allowed = lax.broadcasted_iota(jnp.int32, (block_rows, keys), 1) <= query_pos
        for h in range(broad + narrow):
            if h < broad:
                q = qb_ref[:, h * wb : (h + 1) * wb]
                key = jnp.concatenate([kb[:, h * DB : (h + 1) * DB], rot], axis=1)
                v = vb[:, h * DB : (h + 1) * DB]
                scale = wb ** (-0.5)
            else:
                n = h - broad
                q = qn_ref[:, n * wn : (n + 1) * wn]
                key = jnp.concatenate([kn[:, n * DN : (n + 1) * DN], rot], axis=1)
                v = vn
                scale = wn ** (-0.5)
            score = scale * lax.dot_general(
                q, key, (((1,), (1,)), ((), ())), preferred_element_type=f32
            )
            if k == 0:
                score = jnp.where(allowed, score, masked_score)
                new_max = jnp.max(score, axis=-1, keepdims=True)
                e = jnp.where(allowed, jnp.exp(score - new_max), 0.0)
                new_sum = jnp.sum(e, axis=-1, keepdims=True)
                acc_ref[h] = jnp.dot(e.astype(bf16), v, preferred_element_type=f32)
            else:
                old_max = top_ref[h]
                new_max = jnp.maximum(old_max, jnp.max(score, axis=-1, keepdims=True))
                e = jnp.exp(score - new_max)
                factor = jnp.exp(old_max - new_max)
                new_sum = sum_ref[h] * factor + jnp.sum(e, axis=-1, keepdims=True)
                acc_ref[h] = acc_ref[h] * factor + jnp.dot(
                    e.astype(bf16), v, preferred_element_type=f32
                )
            top_ref[h] = new_max
            sum_ref[h] = new_sum

    def up_in_z(i, at):
        held = up_at(core, at * cols + y)
        arrive(held, base["up_z"] + at)
        send(held, held, peer_y, base["up_y"] + 1 + i)
        send(held, held, peer_c, base["up_c"] + 1 + i)

    def down_in_z(at, cond=None):
        for i in range(2):
            held = down_half(down_at(core, at), i)
            if cond is None:
                arrive(held, base["down_z"] + 2 * at + i)
            else:
                pl.when(cond)(lambda: arrive(held, base["down_z"] + 2 * at + i))
            send(held, held, peer_y, base["down_y"] + 2 * at + i, cond)
            send(held, held, peer_c, base["down_c"] + 4 * at + i, cond)

    lat_in_y(0)
    lat_in_z(1)
    lat_in_z(2)
    lat_in_z(3)
    lat_in_x(0)
    send(cut(up_hbm, z), up_at(core, s), peer_y, base["up_y"])
    send(cut(up_hbm, z), up_at(core, s), peer_c, base["up_c"])
    own_copy.wait()
    attend(0)
    lat_in_y(1)
    lat_in_y(2)
    lat_in_y(3)
    lat_in_x(1)
    up_in_z(2, mate)
    for i in range(2):
        held = down_half(cut(down_hbm, z), i)
        own_half = down_half(down_at(core, z), i)
        send(held, own_half, peer_y, base["down_y"] + 2 * z + i)
        send(held, own_half, peer_c, base["down_c"] + 4 * z + i)
    guarded(1, lambda: attend(1))
    lat_in_x(2)
    lat_in_x(3)
    guarded(2, lambda: attend(2))
    guarded(3, lambda: attend(3))

    parts = [acc_ref[h] / sum_ref[h] for h in range(broad + narrow)]
    for h in range(broad):
        for i in range(tp):
            attn[i, :, h * DB : (h + 1) * DB] = parts[h][i * share : (i + 1) * share].astype(bf16)
    column = lax.broadcasted_iota(jnp.int32, parts[broad].shape, 1)
    merged = parts[broad]
    for n in range(1, narrow):
        merged = jnp.where(column >= n * DN, parts[broad + n], merged)
    for i in range(tp):
        attn[i, :, broad * DB :] = merged[i * share : (i + 1) * share].astype(bf16)

    turned_to = ((t_x, peer_x), (t_both, peer_b), (t_core, peer_c))
    for i, (at, peer) in enumerate(turned_to):
        send(attn.at[at], heads.at[t], peer, base["heads"] + i)
    heads[t] = attn[t]
    for copy in outs:
        copy.wait()
    for i, (at, _) in enumerate(turned_to):
        arrive(heads.at[at], base["heads"] + i)

    down_in_z(mate, edge)
    broad_width = kb_ref.shape[1]
    narrow_width = kn_ref.shape[1]
    projected = jnp.zeros((share, ob.shape[1]), f32)
    for i in range(tp):
        projected = projected + jnp.dot(
            heads[i, :, :broad_width],
            ob[i * broad_width : (i + 1) * broad_width],
            preferred_element_type=f32,
        )
        projected = projected + jnp.dot(
            heads[i, :, broad_width:],
            on[i * narrow_width : (i + 1) * narrow_width],
            preferred_element_type=f32,
        )
    mixed = (
        resid_ref[pl.ds(pl.multiple_of(t * share, 16), share), :].astype(f32)
        + rms_scale(projected, post_ref[...])
    ).astype(bf16)
    rows[0, z] = rms_scale(mixed.astype(f32), gain_ref[...]).astype(bf16)

    def row_piece(side, at, c):
        return rows.at[side, at, pl.ds(c * row_step, row_step)]

    crossing = []
    for dest in (gate, mate):
        for c in range(row_chunks):
            held = row_piece(0, z, c)
            send(held, held, line(dest), base["row_z"] + z * row_chunks + c)
            if dest is gate:
                crossing.append(started.pop()[1])
                started.append((edge, crossing[-1]))
                send(held, row_piece(1, z, c), peer_x, base["row_x"] + c)
    send_down(mate, edge)
    send_down(gate, z == 3)

    def up_in_y(i, at):
        held = up_at(core, at * cols + 1 - y)
        arrive(held, base["up_y"] + i)
        send(held, held, peer_c, base["up_c"] + lines + i)

    def row_in(i, at):
        for c in range(row_chunks):
            held = row_piece(0, at, c)
            index = base["row_z"] + at * row_chunks + c
            arrive(held, index)
            if i < 2:
                send(held, held, line(mate), index, inner)
            send(held, row_piece(1, at, c), peer_x, base["row_x"] + (1 + i) * row_chunks + c)

    up_in_z(0, gate)
    up_in_z(1, outer)
    row_in(2, mate)
    row_in(0, gate)
    row_in(1, outer)
    @pl.when(inner)
    def _():
        for copy in crossing:
            copy.wait_send()
        pl.semaphore_signal(pair_sem, inc=1, device_id=peer_c, device_id_type=mesh_id)
        pl.semaphore_wait(pair_sem, 1)

    send_down(gate, z == 1)
    send_down(outer, inner)
    steps = (z,) + far
    down_in_z(mate, inner)
    down_in_z(gate, edge)
    for i, at in enumerate(steps):
        up_in_y(i, at)
    own[0].wait()
    for i, at in enumerate(steps):
        arrive(up_at(1 - core, at * cols + y), base["up_c"] + i)
        arrive(up_at(1 - core, at * cols + 1 - y), base["up_c"] + lines + i)

    deep = sp * up.shape[2]

    def raise_rows(j):
        block_in = rows[j].reshape(lines * share, rows.shape[3])
        for origin in range(2):
            product = jnp.dot(
                block_in, up[origin].reshape(deep, width), preferred_element_type=f32
            )
            hidden_ref[
                j * lines * share : (j + 1) * lines * share, origin * width : (origin + 1) * width
            ] = jnp.square(jnp.maximum(product, 0.0)).astype(bf16)

    raise_rows(0)
    send_down(gate, z == 0)
    send_down(outer, edge)

    def down_in_y(at):
        for i in range(2):
            held = down_half(down_at(core, at, True), i)
            arrive(held, base["down_y"] + 2 * at + i)
            send(held, held, peer_c, base["down_c"] + 4 * at + 2 + i)

    units = (gate, outer, mate, z)

    deep_part = down.shape[3]
    early = (lines - 1) * half
    late = (lines - 1) * (1 - half)

    def sibling_in(at, flipped):
        for i in range(2):
            held = down_half(down_at(1 - core, at, flipped), i)
            arrive(held, base["down_c"] + 4 * at + 2 * flipped + i)

    def columns_of(start, count):
        if not isinstance(start, int):
            start = pl.multiple_of(start, lane_tile)
        return pl.ds(start, count)

    def lower(weights, columns):
        total = None
        for origin in range(2):
            product = lax.dot_general(
                hidden_ref[:, origin * width : (origin + 1) * width],
                weights(origin),
                (((1,), (1,)), ((), ())),
                preferred_element_type=f32,
            )
            total = product if total is None else total + product
        total = total.reshape(2, lines, share, total.shape[1])
        part[:, :, columns] = total[0]
        x_send[:, :, columns] = total[1].astype(bf16)

    def send_sums(group, columns):
        for i, at in enumerate(units):
            send(
                x_send.at[at, :, columns],
                x_got.at[at, :, columns],
                peer_x,
                base["sum_x"] + group * lines + i,
            )

    def lower_middle():
        for at in (1, 2):
            sibling_in(at, 0)
            sibling_in(at, 1)
        wide = 2 * cols * deep_part
        columns = pl.ds(cols * deep_part, wide)
        lower(lambda origin: down[origin, 1:3].reshape(wide, width), columns)
        send_sums(0, columns)
        return 0, columns

    def lower_edge(at, flipped):
        sibling_in(at, flipped)
        side = (1 - y) if flipped else y
        columns = columns_of((at * cols + side) * deep_part, deep_part)
        lower(lambda origin: down[origin, at, side], columns)
        group = 1 + 2 * (at // (lines - 1)) + flipped
        send_sums(group, columns)
        return group, columns

    def pair(group, columns, i):
        at = units[i]
        arrive(x_got.at[at, :, columns], base["sum_x"] + group * lines + i)
        return part[at, :, columns] + x_got[at, :, columns].astype(f32)

    def sum_copy(i, got, peer, index, cond, columns):
        copy = pltpu.make_async_remote_copy(
            src_ref=z_send.at[i, :, columns],
            dst_ref=got.at[:, columns],
            send_sem=send_sem.at[len(started)],
            recv_sem=recv_sem.at[index],
            device_id=peer,
            device_id_type=mesh_id,
        )
        started.append((cond, copy))
        return copy

    def combine(group, columns):
        near = [
            sum_copy(
                i, r_got.at[i], line(mate), base["sum_r"] + group * 2 + i, edge, columns
            )
            for i in range(2)
        ]
        own_sum = sum_copy(2, m_got, line(mate), base["sum_m"] + group, None, columns)
        across = [
            sum_copy(i, f_got, line(units[i]), base["sum_f"] + group, inner, columns)
            for i in range(2)
        ]

        def mate_part():
            z_send[2, :, columns] = pair(group, columns, 2).astype(bf16)
            own_sum.start()

        def edge_part():
            for i in range(2):
                z_send[i, :, columns] = pair(group, columns, i).astype(bf16)
                near[i].start()
            mate_part()

        def inner_part():
            for i in range(2):
                value = pair(group, columns, i)
                got = r_got.at[i, :, columns]
                arrive(got, base["sum_r"] + group * 2 + i)
                z_send[i, :, columns] = (value + got[...].astype(f32)).astype(bf16)
                across[i].start()
            mate_part()

        return edge_part, inner_part

    def finish(group, columns):
        value = pair(group, columns, 3)
        arrive(m_got.at[:, columns], base["sum_m"] + group)
        value = value + m_got[:, columns].astype(f32)
        arrive(f_got.at[:, columns], base["sum_f"] + group)
        ffn_ref[:, columns] = value + f_got[:, columns].astype(f32)

    for i, at in enumerate((z, gate, outer, mate)):
        for c in range(row_chunks):
            arrive(row_piece(1, at, c), base["row_x"] + i * row_chunks + c)
    raise_rows(1)
    own[1].wait()
    down_in_y(early)
    made = [lower_edge(early, 0), lower_edge(early, 1)]
    down_in_z(gate, inner)
    down_in_y(1)
    down_in_y(2)
    made.append(lower_middle())
    steps_of = [combine(*item) for item in made]
    pl.when(edge)(steps_of[0][0])
    pl.when(edge)(steps_of[1][0])
    down_in_z(outer)
    made.append(lower_edge(late, 0))
    steps_of.append(combine(*made[3]))
    pl.when(edge)(steps_of[2][0])
    down_in_y(late)
    made.append(lower_edge(late, 1))
    steps_of.append(combine(*made[4]))
    for item in steps_of[:3]:
        pl.when(inner)(item[1])
    for item in steps_of[3:]:
        pl.when(edge)(item[0])
        pl.when(inner)(item[1])
    finish(*made[2])
    for at, flipped in ((early, 0), (early, 1), (late, 0), (late, 1)):
        side = (1 - y) if flipped else y
        finish(
            1 + 2 * (at // (lines - 1)) + flipped,
            columns_of((at * cols + side) * deep_part, deep_part),
        )
    out_ref[...] = (mixed.astype(f32) + rms_scale(ffn_ref[...], last_ref[...])).astype(bf16)
    for cond, copy in started:
        if cond is None:
            copy.wait_send()
        else:
            pl.when(cond)(lambda: copy.wait_send())


def fast_local(
    resid,
    query_broad,
    query_narrow,
    latent,
    key_rope,
    latent_gain,
    key_up_broad,
    value_up_broad,
    key_up_narrow,
    value_up_narrow,
    out_broad,
    out_narrow,
    post_gain,
    ffn_gain,
    up_weight,
    down_weight,
    ffn_out_gain,
):
    sp = lax.axis_size("sp")
    tp = lax.axis_size("tp")
    cols = row_parts
    lines = sp // cols
    s = lax.axis_index("sp")
    z = s // cols
    y = s % cols
    local_rows = resid.shape[0]
    share_rows = local_rows // tp
    query_pos = s * local_rows + jnp.arange(local_rows, dtype=jnp.int32)
    rope_width = key_rope.shape[1]
    bf16 = jnp.bfloat16

    frequency = rope_base ** (-2.0 * jnp.arange(rope_width // 2, dtype=jnp.float32) / rope_width)
    angles = query_pos.astype(jnp.float32)[:, None] * frequency[None, :]
    cosine, sine = jnp.cos(angles), jnp.sin(angles)
    table = jnp.concatenate([cosine, cosine, -sine, sine], axis=1)
    half_rows = local_rows // 2
    both_width = latent.shape[1] + rope_width
    broad_width = key_up_broad.shape[1]
    narrow_width = key_up_narrow.shape[1]
    width = broad_width + narrow_width
    deep = resid.shape[1]
    slice_width = up_weight.shape[1] // lines
    vmem = pl.BlockSpec(memory_space=pltpu.VMEM)
    anywhere = pl.BlockSpec(memory_space=pl.ANY)
    chunks = 5
    heads = broad_width // DB + narrow_width // DN
    _, sems = sem_layout(lines, tp, chunks, share_rows // 16)
    f32 = jnp.float32
    return pl.pallas_call(
        functools.partial(layer_kernel, sp, tp),
        out_shape=jax.ShapeDtypeStruct((share_rows, deep), bf16),
        in_specs=[vmem] * 11 + [anywhere] * 2 + [vmem] * 3 + [anywhere] * 2,
        out_specs=vmem,
        scratch_shapes=[
            pltpu.VMEM((share_rows, both_width), bf16),
            pltpu.VMEM(query_broad.shape, bf16),
            pltpu.VMEM(query_narrow.shape, bf16),
            pltpu.VMEM((sp, tp, share_rows, both_width), bf16),
            pltpu.VMEM((heads, local_rows, 1), f32),
            pltpu.VMEM((heads, local_rows, 1), f32),
            pltpu.VMEM((heads, local_rows, lane_tile), f32),
            pltpu.VMEM((tp, share_rows, width), bf16),
            pltpu.VMEM((tp, share_rows, width), bf16),
            pltpu.VMEM(out_broad.shape, bf16),
            pltpu.VMEM(out_narrow.shape, bf16),
            pltpu.VMEM((2, sp, up_weight.shape[0], slice_width), bf16),
            pltpu.VMEM((2, lines, cols, down_weight.shape[0], slice_width), bf16),
            pltpu.VMEM((2, lines, share_rows, deep), bf16),
            pltpu.VMEM((2 * lines * share_rows, 2 * slice_width), bf16),
            pltpu.VMEM((lines, share_rows, deep), f32),
            pltpu.VMEM((lines, share_rows, deep), bf16),
            pltpu.VMEM((lines, share_rows, deep), bf16),
            pltpu.VMEM((3, share_rows, deep), bf16),
            pltpu.VMEM((2, share_rows, deep), bf16),
            pltpu.VMEM((share_rows, deep), bf16),
            pltpu.VMEM((share_rows, deep), bf16),
            pltpu.VMEM((share_rows, deep), f32),
            pltpu.SemaphoreType.DMA((2 * sems,)),
            pltpu.SemaphoreType.DMA((sems,)),
            pltpu.SemaphoreType.DMA((5,)),
            pltpu.SemaphoreType.REGULAR,
        ],
        compiler_params=pltpu.CompilerParams(
            collective_id=0, has_side_effects=True, vmem_limit_bytes=60 * 2**20
        ),
    )(
        latent,
        key_rope,
        table,
        latent_gain[None],
        query_broad,
        query_narrow,
        resid,
        key_up_broad,
        value_up_broad,
        key_up_narrow,
        value_up_narrow,
        out_broad,
        out_narrow,
        post_gain[None],
        ffn_gain[None],
        ffn_out_gain[None],
        up_weight,
        down_weight,
    )


def solution(mesh):
    in_specs = (
        P("sp", None),
        P("sp", "tp"),
        P("sp", "tp"),
        P("sp", None),
        P("sp", None),
        P(),
        P(None, "tp"),
        P(None, "tp"),
        P(None, "tp"),
        P(None, "tp"),
        P(),
        P(),
        P(),
        P(),
        P("sp", "tp"),
        P("sp", "tp"),
        P(),
    )
    out_specs = P(("sp", "tp"), None)
    sp = mesh.shape["sp"]
    tp = mesh.shape["tp"]

    def whole(*args):
        hidden = args[14].shape[1] // tp
        rows = args[0].shape[0] // sp
        lines = sp // row_parts
        fits = (
            sp % row_parts == 0
            and tp & (tp - 1) == 0
            and tp == 4
            and lines == 4
            and hidden % (lines * lane_tile) == 0
            and args[0].shape[1] % (2 * lane_tile * sp) == 0
            and rows % (16 * tp) == 0
        )
        body = fast_local if fits else local
        return jax.shard_map(
            body, mesh=mesh, in_specs=in_specs, out_specs=out_specs, check_vma=False
        )(*args)

    return whole
```

```python
import functools
import math

import jax
import jax.numpy as jnp
import numpy as np
from jax import lax
from jax.experimental import pallas as pl
from jax.experimental.pallas import tpu as pltpu
from jax.sharding import PartitionSpec as P

DB = 128
DN = 64


norm_eps = 1e-06
rope_base = 500000.0
masked_score = -1e30


def rotate(values, positions):
    full_width = values.shape[-1]
    half_width = full_width // 2
    frequency = rope_base ** (-2.0 * jnp.arange(half_width, dtype=jnp.float32) / full_width)
    angles = positions.astype(jnp.float32)[:, None] * frequency[None, :]
    angle_shape = (angles.shape[0],) + (1,) * (values.ndim - 2) + (half_width,)
    cosine = jnp.cos(angles).reshape(angle_shape)
    sine_part = jnp.sin(angles).reshape(angle_shape)
    leading = values[..., :half_width]
    trailing = values[..., half_width:]
    return jnp.concatenate(
        [leading * cosine - trailing * sine_part, trailing * cosine + leading * sine_part], axis=-1
    )


def rms_scale(values, norm_gain):
    return (
        values * lax.rsqrt(jnp.mean(values * values, axis=-1, keepdims=True) + norm_eps) * norm_gain
    )


def group_update(
    running, nope_query, rope_query, key_rows, key_rot, value_rows, score_scale, allowed
):
    old_max, old_sum, old_acc = running
    scores = jnp.einsum("qhd,khd->hqk", nope_query, key_rows, preferred_element_type=jnp.float32)
    scores = scores + jnp.einsum(
        "qhd,kd->hqk", rope_query, key_rot, preferred_element_type=jnp.float32
    )
    scores = jnp.where(allowed, scores * score_scale, masked_score)
    new_max = jnp.maximum(old_max, jnp.max(scores, axis=-1))
    exponent = jnp.where(allowed, jnp.exp(scores - new_max[:, :, None]), 0.0)
    factor = jnp.exp(old_max - new_max)
    new_sum = old_sum * factor + jnp.sum(exponent, axis=-1)
    weighted = jnp.einsum(
        "hqk,khd->qhd",
        exponent.astype(jnp.bfloat16),
        value_rows,
        preferred_element_type=jnp.float32,
    )
    new_acc = old_acc * jnp.transpose(factor)[:, :, None] + weighted
    return (new_max, new_sum, new_acc)


def local(
    resid,
    query_broad,
    query_narrow,
    latent,
    key_rope,
    latent_gain,
    key_up_broad,
    value_up_broad,
    key_up_narrow,
    value_up_narrow,
    out_broad,
    out_narrow,
    post_gain,
    ffn_gain,
    up_weight,
    down_weight,
    ffn_out_gain,
):
    local_rows = resid.shape[0]
    head_parts = lax.axis_size("tp")
    share_rows = local_rows // head_parts
    row_offset = lax.axis_index("sp") * local_rows
    last_query = row_offset + local_rows - 1
    query_pos = row_offset + jnp.arange(local_rows, dtype=jnp.int32)
    rope_width = key_rope.shape[1]
    broad_count = key_up_broad.shape[1] // DB
    narrow_count = key_up_narrow.shape[1] // DN
    broad_heads = query_broad.reshape(local_rows, broad_count, DB + rope_width)
    broad_nope = broad_heads[:, :, :DB]
    broad_rope = rotate(broad_heads[:, :, DB:].astype(jnp.float32), query_pos).astype(jnp.bfloat16)
    narrow_heads = query_narrow.reshape(local_rows, narrow_count, DN + rope_width)
    narrow_nope = narrow_heads[:, :, :DN]
    narrow_rope = rotate(narrow_heads[:, :, DN:].astype(jnp.float32), query_pos).astype(
        jnp.bfloat16
    )
    broad_scale = (DB + rope_width) ** (-0.5)
    narrow_scale = (DN + rope_width) ** (-0.5)

    def attend(running, latent_rows, rope_rows, first_row):
        key_count = latent_rows.shape[0]
        key_pos = first_row + jnp.arange(key_count, dtype=jnp.int32)
        latent_normed = rms_scale(latent_rows.astype(jnp.float32), latent_gain).astype(jnp.bfloat16)

        def expand(weight, head_size):
            product = jnp.dot(latent_normed, weight, preferred_element_type=jnp.float32)
            return product.astype(jnp.bfloat16).reshape(key_count, -1, head_size)

        key_rot = rotate(rope_rows.astype(jnp.float32), key_pos).astype(jnp.bfloat16)
        allowed = (key_pos[None, :] <= query_pos[:, None])[None]
        broad_state = group_update(
            running[0],
            broad_nope,
            broad_rope,
            expand(key_up_broad, DB),
            key_rot,
            expand(value_up_broad, DB),
            broad_scale,
            allowed,
        )
        narrow_state = group_update(
            running[1],
            narrow_nope,
            narrow_rope,
            expand(key_up_narrow, DN),
            key_rot,
            expand(value_up_narrow, DN),
            narrow_scale,
            allowed,
        )
        return (broad_state, narrow_state)

    def fresh(head_count, head_size):
        return (
            jnp.full((head_count, local_rows), masked_score, jnp.float32),
            jnp.zeros((head_count, local_rows), jnp.float32),
            jnp.zeros((local_rows, head_count, head_size), jnp.float32),
        )

    initial = (fresh(broad_count, DB), fresh(narrow_count, DN))
    latent_piece = lax.all_gather(latent, "sp", axis=0, tiled=True)
    rope_piece = lax.all_gather(key_rope, "sp", axis=0, tiled=True)
    piece_rows = latent_piece.shape[0]
    block_rows = math.gcd(piece_rows, 1024)

    def one_block(block_index, carried):
        begin = block_index * block_rows
        latent_block = lax.dynamic_slice_in_dim(latent_piece, begin, block_rows, 0)
        rope_block = lax.dynamic_slice_in_dim(rope_piece, begin, block_rows, 0)

        def unchanged(kept_state):
            return kept_state

        def updated(kept_state):
            return attend(kept_state, latent_block, rope_block, begin)

        return lax.cond(begin > last_query, unchanged, updated, carried)

    final_state = lax.fori_loop(0, piece_rows // block_rows, one_block, initial)

    def finish(running):
        run_max, run_sum, run_acc = running
        return (
            (run_acc / jnp.transpose(run_sum)[:, :, None])
            .astype(jnp.bfloat16)
            .reshape(local_rows, -1)
        )

    attn_broad = finish(final_state[0])
    attn_narrow = finish(final_state[1])
    rows_broad, rows_narrow = (
        lax.all_to_all(attn_broad, "tp", split_axis=0, concat_axis=1, tiled=True),
        lax.all_to_all(attn_narrow, "tp", split_axis=0, concat_axis=1, tiled=True),
    )
    projected = jnp.dot(rows_broad, out_broad, preferred_element_type=jnp.float32) + jnp.dot(
        rows_narrow, out_narrow, preferred_element_type=jnp.float32
    )
    own_resid = lax.dynamic_slice_in_dim(resid, lax.axis_index("tp") * share_rows, share_rows, 0)
    mixed = (own_resid.astype(jnp.float32) + rms_scale(projected, post_gain)).astype(jnp.bfloat16)
    normed = rms_scale(mixed.astype(jnp.float32), ffn_gain).astype(jnp.bfloat16)
    up_full, down_full = (
        lax.all_gather(up_weight, "sp", axis=0, tiled=True),
        lax.all_gather(down_weight, "sp", axis=0, tiled=True),
    )
    hidden = jnp.square(
        jax.nn.relu(
            jnp.dot(
                lax.all_gather(normed, "tp", axis=0, tiled=True),
                up_full,
                preferred_element_type=jnp.float32,
            )
        )
    ).astype(jnp.bfloat16)
    ffn = lax.psum_scatter(
        lax.dot_general(
            hidden, down_full, (((1,), (1,)), ((), ())), preferred_element_type=jnp.float32
        ).astype(jnp.bfloat16),
        "tp",
        scatter_dimension=0,
        tiled=True,
    ).astype(jnp.float32)
    return (mixed.astype(jnp.float32) + rms_scale(ffn, ffn_out_gain)).astype(jnp.bfloat16)

lane_tile = 128
row_parts = 2
mesh_id = pl.DeviceIdType.MESH


def sem_layout(lines, tp, chunks, row_chunks):
    sizes = {
        "lat_z": lines,
        "lat_y": lines,
        "lat_x": 2 * lines,
        "lat_c": 4 * lines,
        "up_z": lines,
        "up_y": lines,
        "up_c": 2 * lines,
        "down_z": 2 * lines,
        "down_y": 2 * lines,
        "down_c": 4 * lines,
        "heads": tp,
        "row_z": lines * row_chunks,
        "row_x": lines * row_chunks,
        "sum_x": chunks * lines,
        "sum_r": chunks * 2,
        "sum_m": chunks,
        "sum_f": chunks,
    }
    base, total = {}, 0
    for name, size in sizes.items():
        base[name] = total
        total += size
    return base, total


def layer_kernel(
    sp,
    tp,
    latent_ref,
    key_rope_ref,
    frequency_ref,
    latent_gain_ref,
    qb_hbm,
    qn_hbm,
    resid_hbm,
    kb_hbm,
    vb_hbm,
    kn_hbm,
    vn_hbm,
    ob_hbm,
    on_hbm,
    post_ref,
    gain_ref,
    last_ref,
    up_hbm,
    down_hbm,
    out_ref,
    qb_in,
    qn_in,
    resid_ref,
    kb_ref,
    vb_ref,
    kn_ref,
    vn_ref,
    mine_ref,
    qb_ref,
    qn_ref,
    lat,
    top_ref,
    sum_ref,
    acc_ref,
    attn,
    heads,
    ob,
    on,
    up,
    down,
    rows,
    hidden_ref,
    part,
    x_send,
    x_got,
    z_send,
    r_got,
    m_got,
    f_got,
    ffn_ref,
    send_sem,
    recv_sem,
    local_sem,
    pair_sem,
):
    cols = row_parts
    lines = sp // cols
    chunks = 5
    s = lax.axis_index("sp")
    t = lax.axis_index("tp")
    z = s // cols
    y = s % cols
    core = t % 2
    x = t // 2
    t_core = 2 * x + 1 - core
    t_x = 2 * (1 - x) + core
    t_both = 2 * (1 - x) + 1 - core
    s_y = z * cols + 1 - y
    half = z // 2
    mate = z + 1 - 2 * (z % 2)
    gate = 2 - half
    outer = 3 * (1 - half)
    inner = (z == 1) | (z == 2)
    edge = (z == 0) | (z == 3)
    bf16 = jnp.bfloat16
    f32 = jnp.float32
    block_rows = latent_ref.shape[0]
    share = block_rows // tp
    width = up.shape[3]
    row_step = 16
    row_chunks = share // row_step
    base, _ = sem_layout(lines, tp, chunks, row_chunks)

    def line(at):
        return (at * cols + y, t)

    peer_y, peer_x, peer_c, peer_b = (s_y, t), (s, t_x), (s, t_core), (s, t_both)
    peers = [line(mate), line(gate), line(outer), peer_y, peer_x, peer_c, peer_b]
    barrier = pltpu.get_barrier_semaphore()
    for peer in peers:
        pl.semaphore_signal(barrier, inc=1, device_id=peer, device_id_type=mesh_id)

    locals_ = []

    def bring(src, dst):
        copy = pltpu.make_async_copy(src, dst, local_sem.at[len(locals_)])
        copy.start()
        locals_.append(copy)
        return copy

    rope = key_rope_ref.shape[0]
    half_rope = rope // 2

    def table(first, count):
        row = lax.broadcasted_iota(jnp.int32, (count, rope), 0) + first
        angles = row.astype(f32) * frequency_ref[...]
        lane = lax.broadcasted_iota(jnp.int32, (count, rope), 1)
        sine = jnp.sin(angles)
        return jnp.cos(angles), jnp.where(lane < half_rope, -sine, sine)

    def turn(values, tables):
        values = values.astype(f32)
        swapped = jnp.concatenate([values[:, half_rope:], values[:, :half_rope]], axis=1)
        return (values * tables[0] + swapped * tables[1]).astype(bf16)

    latent_width = latent_ref.shape[1]
    mine_rows = pl.ds(pl.multiple_of(t * share, 16), share)
    mine_ref[:, :latent_width] = rms_scale(
        latent_ref[mine_rows, :].astype(f32), latent_gain_ref[...]
    ).astype(bf16)
    picked = lax.broadcasted_iota(jnp.int32, (share, block_rows), 1) == (
        lax.broadcasted_iota(jnp.int32, (share, block_rows), 0) + t * share
    )
    key_rows = lax.dot_general(
        jnp.where(picked, 1.0, 0.0).astype(bf16),
        key_rope_ref[...],
        (((1,), (1,)), ((), ())),
        preferred_element_type=f32,
    )
    mine_ref[:, latent_width:] = turn(key_rows, table(s * block_rows + t * share, share))
    pl.semaphore_wait(barrier, len(peers))

    started = []

    def send(src, dst, peer, recv, cond=None):
        copy = pltpu.make_async_remote_copy(
            src_ref=src,
            dst_ref=dst,
            send_sem=send_sem.at[len(started)],
            recv_sem=recv_sem.at[recv],
            device_id=peer,
            device_id_type=mesh_id,
        )
        started.append((cond, copy))
        if cond is None:
            copy.start()
        else:
            pl.when(cond)(lambda: copy.start())

    def arrive(dst, recv):
        pltpu.make_async_remote_copy(
            src_ref=dst,
            dst_ref=dst,
            send_sem=send_sem.at[0],
            recv_sem=recv_sem.at[recv],
            device_id=peer_c,
            device_id_type=mesh_id,
        ).wait_recv()

    def block(k, flipped):
        return (z - k) * cols + ((1 - y) if flipped else y)

    for k in range(lines - 1, 0, -1):
        send(mine_ref, lat.at[s, t], line(z + k), base["lat_z"] + k, z + k < lines)
    send(mine_ref, lat.at[s, t], peer_y, base["lat_y"])
    send(mine_ref, lat.at[s, t], peer_x, base["lat_x"])
    send(mine_ref, lat.at[s, t], peer_c, base["lat_c"])
    own_copy = bring(mine_ref, lat.at[s, t])

    def cut(ref, at):
        return ref.at[:, pl.ds(pl.multiple_of(at * width, width), width)]

    far = (gate, outer, mate)

    def up_at(origin, at):
        return up.at[origin, at]

    def down_at(origin, at, flipped=False):
        return down.at[origin, at, (1 - y) if flipped else y]

    def send_down(dest, cond=None):
        for i in range(2):
            send(
                down_half(cut(down_hbm, dest), i),
                down_half(down_at(core, z), i),
                line(dest),
                base["down_z"] + 2 * z + i,
                cond,
            )

    def down_half(ref, i):
        rows_half = down.shape[3] // 2
        return ref.at[pl.ds(i * rows_half, rows_half)]

    def send_up(dest, cond):
        send(cut(up_hbm, dest), up_at(core, s), line(dest), base["up_z"] + z, cond)

    send_up(mate, edge)
    for dest in far:
        send_up(dest, None if dest is not mate else inner)
    send_down(mate, inner)
    send_down(gate, z == 2)
    own = [bring(cut(up_hbm, z), up_at(core, s))]
    own.append(bring(cut(down_hbm, z), down_at(core, z)))
    queries = [bring(qb_hbm, qb_in), bring(qn_hbm, qn_in)]
    expands = [
        bring(kb_hbm, kb_ref),
        bring(vb_hbm, vb_ref),
        bring(kn_hbm, kn_ref),
        bring(vn_hbm, vn_ref),
    ]
    outs = [bring(ob_hbm, ob), bring(on_hbm, on), bring(resid_hbm, resid_ref)]
    query_table = table(s * block_rows, block_rows)
    for copy in queries:
        copy.wait()

    for queries, turned, size in ((qb_in, qb_ref, DB), (qn_in, qn_ref, DN)):
        step = size + rope
        for h in range(queries.shape[1] // step):
            middle = h * step + size
            turned[:, h * step : middle] = queries[:, h * step : middle]
            turned[:, middle : middle + rope] = turn(
                queries[:, middle : middle + rope], query_table
            )

    def when(k):
        return None if k == 0 else z >= k

    def guarded(k, body):
        if k == 0:
            body()
        else:
            pl.when(z >= k)(body)

    def lat_in_z(k):
        held = lat.at[block(k, False), t]
        guarded(k, lambda: arrive(held, base["lat_z"] + k))
        send(held, held, peer_y, base["lat_y"] + k, when(k))
        send(held, held, peer_x, base["lat_x"] + 2 * k, when(k))
        send(held, held, peer_c, base["lat_c"] + 4 * k, when(k))

    def lat_in_y(k):
        held = lat.at[block(k, True), t]
        guarded(k, lambda: arrive(held, base["lat_y"] + k))
        send(held, held, peer_x, base["lat_x"] + 2 * k + 1, when(k))
        send(held, held, peer_c, base["lat_c"] + 4 * k + 1, when(k))

    def lat_in_x(k):
        for i, flipped in enumerate((False, True)):
            held = lat.at[block(k, flipped), t_x]
            guarded(k, lambda: arrive(held, base["lat_x"] + 2 * k + i))
            send(held, held, peer_c, base["lat_c"] + 4 * k + 2 + i, when(k))

    broad = kb_ref.shape[1] // DB
    narrow = kn_ref.shape[1] // DN
    wb = DB + rope
    wn = DN + rope
    keys = cols * block_rows

    def attend(k):
        for i, flipped in enumerate((False, True)):
            arrive(lat.at[block(k, flipped), t_core], base["lat_c"] + 4 * k + i)
            arrive(lat.at[block(k, flipped), t_both], base["lat_c"] + 4 * k + 2 + i)
        both = lat[pl.ds((z - k) * cols, cols)].reshape(keys, latent_width + rope)
        normed = both[:, :latent_width]
        rot = both[:, latent_width:]

        def expand(ref):
            return jnp.dot(normed, ref[...], preferred_element_type=f32).astype(bf16)

        kb, vb, kn, vn = expand(kb_ref), expand(vb_ref), expand(kn_ref), expand(vn_ref)
        if k == 0:
            query_pos = y * block_rows + lax.broadcasted_iota(jnp.int32, (block_rows, keys), 0)
            allowed = lax.broadcasted_iota(jnp.int32, (block_rows, keys), 1) <= query_pos
        for h in range(broad + narrow):
            if h < broad:
                q = qb_ref[:, h * wb : (h + 1) * wb]
                key = jnp.concatenate([kb[:, h * DB : (h + 1) * DB], rot], axis=1)
                v = vb[:, h * DB : (h + 1) * DB]
                scale = wb ** (-0.5)
            else:
                n = h - broad
                q = qn_ref[:, n * wn : (n + 1) * wn]
                key = jnp.concatenate([kn[:, n * DN : (n + 1) * DN], rot], axis=1)
                v = vn
                scale = wn ** (-0.5)
            score = scale * lax.dot_general(
                q, key, (((1,), (1,)), ((), ())), preferred_element_type=f32
            )
            if k == 0:
                score = jnp.where(allowed, score, masked_score)
                new_max = jnp.max(score, axis=-1, keepdims=True)
                e = jnp.where(allowed, jnp.exp(score - new_max), 0.0)
                new_sum = jnp.sum(e, axis=-1, keepdims=True)
                acc_ref[h] = jnp.dot(e.astype(bf16), v, preferred_element_type=f32)
            else:
                old_max = top_ref[h]
                new_max = jnp.maximum(old_max, jnp.max(score, axis=-1, keepdims=True))
                e = jnp.exp(score - new_max)
                factor = jnp.exp(old_max - new_max)
                new_sum = sum_ref[h] * factor + jnp.sum(e, axis=-1, keepdims=True)
                acc_ref[h] = acc_ref[h] * factor + jnp.dot(
                    e.astype(bf16), v, preferred_element_type=f32
                )
            top_ref[h] = new_max
            sum_ref[h] = new_sum

    def up_in_z(i, at):
        held = up_at(core, at * cols + y)
        arrive(held, base["up_z"] + at)
        send(held, held, peer_y, base["up_y"] + 1 + i)
        send(held, held, peer_c, base["up_c"] + 1 + i)

    def down_in_z(at, cond=None):
        for i in range(2):
            held = down_half(down_at(core, at), i)
            if cond is None:
                arrive(held, base["down_z"] + 2 * at + i)
            else:
                pl.when(cond)(lambda: arrive(held, base["down_z"] + 2 * at + i))
            send(held, held, peer_y, base["down_y"] + 2 * at + i, cond)
            send(held, held, peer_c, base["down_c"] + 4 * at + i, cond)

    lat_in_y(0)
    lat_in_z(1)
    lat_in_z(2)
    lat_in_z(3)
    lat_in_x(0)
    send(cut(up_hbm, z), up_at(core, s), peer_y, base["up_y"])
    send(cut(up_hbm, z), up_at(core, s), peer_c, base["up_c"])
    own_copy.wait()
    for copy in expands:
        copy.wait()
    attend(0)
    lat_in_y(1)
    lat_in_y(2)
    lat_in_y(3)
    lat_in_x(1)
    up_in_z(2, mate)
    for i in range(2):
        held = down_half(cut(down_hbm, z), i)
        own_half = down_half(down_at(core, z), i)
        send(held, own_half, peer_y, base["down_y"] + 2 * z + i)
        send(held, own_half, peer_c, base["down_c"] + 4 * z + i)
    guarded(1, lambda: attend(1))
    lat_in_x(2)
    lat_in_x(3)
    guarded(2, lambda: attend(2))
    guarded(3, lambda: attend(3))

    parts = [acc_ref[h] / sum_ref[h] for h in range(broad + narrow)]
    for h in range(broad):
        for i in range(tp):
            attn[i, :, h * DB : (h + 1) * DB] = parts[h][i * share : (i + 1) * share].astype(bf16)
    column = lax.broadcasted_iota(jnp.int32, parts[broad].shape, 1)
    merged = parts[broad]
    for n in range(1, narrow):
        merged = jnp.where(column >= n * DN, parts[broad + n], merged)
    for i in range(tp):
        attn[i, :, broad * DB :] = merged[i * share : (i + 1) * share].astype(bf16)

    turned_to = ((t_x, peer_x), (t_both, peer_b), (t_core, peer_c))
    for i, (at, peer) in enumerate(turned_to):
        send(attn.at[at], heads.at[t], peer, base["heads"] + i)
    heads[t] = attn[t]
    for copy in outs:
        copy.wait()
    for i, (at, _) in enumerate(turned_to):
        arrive(heads.at[at], base["heads"] + i)

    down_in_z(mate, edge)
    broad_width = kb_ref.shape[1]
    narrow_width = kn_ref.shape[1]
    projected = jnp.zeros((share, ob.shape[1]), f32)
    for i in range(tp):
        projected = projected + jnp.dot(
            heads[i, :, :broad_width],
            ob[i * broad_width : (i + 1) * broad_width],
            preferred_element_type=f32,
        )
        projected = projected + jnp.dot(
            heads[i, :, broad_width:],
            on[i * narrow_width : (i + 1) * narrow_width],
            preferred_element_type=f32,
        )
    mixed = (
        resid_ref[pl.ds(pl.multiple_of(t * share, 16), share), :].astype(f32)
        + rms_scale(projected, post_ref[...])
    ).astype(bf16)
    rows[0, z] = rms_scale(mixed.astype(f32), gain_ref[...]).astype(bf16)

    def row_piece(side, at, c):
        return rows.at[side, at, pl.ds(c * row_step, row_step)]

    crossing = []
    for dest in (gate, mate):
        for c in range(row_chunks):
            held = row_piece(0, z, c)
            send(held, held, line(dest), base["row_z"] + z * row_chunks + c)
            if dest is gate:
                crossing.append(started.pop()[1])
                started.append((edge, crossing[-1]))
                send(held, row_piece(1, z, c), peer_x, base["row_x"] + c)
    send_down(mate, edge)
    send_down(gate, z == 3)

    def up_in_y(i, at):
        held = up_at(core, at * cols + 1 - y)
        arrive(held, base["up_y"] + i)
        send(held, held, peer_c, base["up_c"] + lines + i)

    def row_in(i, at):
        for c in range(row_chunks):
            held = row_piece(0, at, c)
            index = base["row_z"] + at * row_chunks + c
            arrive(held, index)
            if i < 2:
                send(held, held, line(mate), index, inner)
            send(held, row_piece(1, at, c), peer_x, base["row_x"] + (1 + i) * row_chunks + c)

    up_in_z(0, gate)
    up_in_z(1, outer)
    row_in(2, mate)
    row_in(0, gate)
    row_in(1, outer)
    @pl.when(inner)
    def _():
        for copy in crossing:
            copy.wait_send()
        pl.semaphore_signal(pair_sem, inc=1, device_id=peer_c, device_id_type=mesh_id)
        pl.semaphore_wait(pair_sem, 1)

    send_down(gate, z == 1)
    send_down(outer, inner)
    steps = (z,) + far
    down_in_z(mate, inner)
    down_in_z(gate, edge)
    send_down(gate, z == 0)
    send_down(outer, edge)
    for i, at in enumerate(steps):
        up_in_y(i, at)
    own[0].wait()
    for i, at in enumerate(steps):
        arrive(up_at(1 - core, at * cols + y), base["up_c"] + i)
        arrive(up_at(1 - core, at * cols + 1 - y), base["up_c"] + lines + i)

    deep = sp * up.shape[2]

    def raise_rows(j):
        block_in = rows[j].reshape(lines * share, rows.shape[3])
        for origin in range(2):
            product = jnp.dot(
                block_in, up[origin].reshape(deep, width), preferred_element_type=f32
            )
            hidden_ref[
                j * lines * share : (j + 1) * lines * share, origin * width : (origin + 1) * width
            ] = jnp.square(jnp.maximum(product, 0.0)).astype(bf16)

    raise_rows(0)

    def down_in_y(at):
        for i in range(2):
            held = down_half(down_at(core, at, True), i)
            arrive(held, base["down_y"] + 2 * at + i)
            send(held, held, peer_c, base["down_c"] + 4 * at + 2 + i)

    units = (gate, outer, mate, z)

    deep_part = down.shape[3]
    early = (lines - 1) * half
    late = (lines - 1) * (1 - half)

    def sibling_in(at, flipped):
        for i in range(2):
            held = down_half(down_at(1 - core, at, flipped), i)
            arrive(held, base["down_c"] + 4 * at + 2 * flipped + i)

    def columns_of(start, count):
        if not isinstance(start, int):
            start = pl.multiple_of(start, lane_tile)
        return pl.ds(start, count)

    def lower(weights, columns):
        total = None
        for origin in range(2):
            product = lax.dot_general(
                hidden_ref[:, origin * width : (origin + 1) * width],
                weights(origin),
                (((1,), (1,)), ((), ())),
                preferred_element_type=f32,
            )
            total = product if total is None else total + product
        total = total.reshape(2, lines, share, total.shape[1])
        part[:, :, columns] = total[0]
        x_send[:, :, columns] = total[1].astype(bf16)

    def send_sums(group, columns):
        for i, at in enumerate(units):
            send(
                x_send.at[at, :, columns],
                x_got.at[at, :, columns],
                peer_x,
                base["sum_x"] + group * lines + i,
            )

    def lower_middle():
        for at in (1, 2):
            sibling_in(at, 0)
            sibling_in(at, 1)
        wide = 2 * cols * deep_part
        columns = pl.ds(cols * deep_part, wide)
        lower(lambda origin: down[origin, 1:3].reshape(wide, width), columns)
        send_sums(0, columns)
        return 0, columns

    def lower_edge(at, flipped):
        sibling_in(at, flipped)
        side = (1 - y) if flipped else y
        columns = columns_of((at * cols + side) * deep_part, deep_part)
        lower(lambda origin: down[origin, at, side], columns)
        group = 1 + 2 * (at // (lines - 1)) + flipped
        send_sums(group, columns)
        return group, columns

    def pair(group, columns, i):
        at = units[i]
        arrive(x_got.at[at, :, columns], base["sum_x"] + group * lines + i)
        return part[at, :, columns] + x_got[at, :, columns].astype(f32)

    def sum_copy(i, got, peer, index, cond, columns):
        copy = pltpu.make_async_remote_copy(
            src_ref=z_send.at[i, :, columns],
            dst_ref=got.at[:, columns],
            send_sem=send_sem.at[len(started)],
            recv_sem=recv_sem.at[index],
            device_id=peer,
            device_id_type=mesh_id,
        )
        started.append((cond, copy))
        return copy

    def combine(group, columns):
        near = [
            sum_copy(
                i, r_got.at[i], line(mate), base["sum_r"] + group * 2 + i, edge, columns
            )
            for i in range(2)
        ]
        own_sum = sum_copy(2, m_got, line(mate), base["sum_m"] + group, None, columns)
        across = [
            sum_copy(i, f_got, line(units[i]), base["sum_f"] + group, inner, columns)
            for i in range(2)
        ]

        def mate_part():
            z_send[2, :, columns] = pair(group, columns, 2).astype(bf16)
            own_sum.start()

        def edge_part():
            for i in range(2):
                z_send[i, :, columns] = pair(group, columns, i).astype(bf16)
                near[i].start()
            mate_part()

        def inner_part():
            for i in range(2):
                value = pair(group, columns, i)
                got = r_got.at[i, :, columns]
                arrive(got, base["sum_r"] + group * 2 + i)
                z_send[i, :, columns] = (value + got[...].astype(f32)).astype(bf16)
                across[i].start()
            mate_part()

        return edge_part, inner_part

    def finish(group, columns):
        value = pair(group, columns, 3)
        arrive(m_got.at[:, columns], base["sum_m"] + group)
        value = value + m_got[:, columns].astype(f32)
        arrive(f_got.at[:, columns], base["sum_f"] + group)
        ffn_ref[:, columns] = value + f_got[:, columns].astype(f32)

    for i, at in enumerate((z, gate, outer, mate)):
        for c in range(row_chunks):
            arrive(row_piece(1, at, c), base["row_x"] + i * row_chunks + c)
    raise_rows(1)
    own[1].wait()
    down_in_y(early)
    made = [lower_edge(early, 0), lower_edge(early, 1)]
    down_in_z(gate, inner)
    down_in_y(1)
    down_in_y(2)
    made.append(lower_middle())
    steps_of = [combine(*item) for item in made]
    pl.when(edge)(steps_of[0][0])
    pl.when(edge)(steps_of[1][0])
    down_in_z(outer)
    made.append(lower_edge(late, 0))
    steps_of.append(combine(*made[3]))
    pl.when(edge)(steps_of[2][0])
    down_in_y(late)
    made.append(lower_edge(late, 1))
    steps_of.append(combine(*made[4]))
    for item in steps_of[:3]:
        pl.when(inner)(item[1])
    for item in steps_of[3:]:
        pl.when(edge)(item[0])
        pl.when(inner)(item[1])
    finish(*made[2])
    for at, flipped in ((early, 0), (early, 1), (late, 0), (late, 1)):
        side = (1 - y) if flipped else y
        finish(
            1 + 2 * (at // (lines - 1)) + flipped,
            columns_of((at * cols + side) * deep_part, deep_part),
        )
    out_ref[...] = (mixed.astype(f32) + rms_scale(ffn_ref[...], last_ref[...])).astype(bf16)
    for cond, copy in started:
        if cond is None:
            copy.wait_send()
        else:
            pl.when(cond)(lambda: copy.wait_send())


def fast_local(
    resid,
    query_broad,
    query_narrow,
    latent,
    key_rope,
    latent_gain,
    key_up_broad,
    value_up_broad,
    key_up_narrow,
    value_up_narrow,
    out_broad,
    out_narrow,
    post_gain,
    ffn_gain,
    up_weight,
    down_weight,
    ffn_out_gain,
):
    sp = lax.axis_size("sp")
    tp = lax.axis_size("tp")
    cols = row_parts
    lines = sp // cols
    local_rows = resid.shape[0]
    share_rows = local_rows // tp
    rope_width = key_rope.shape[1]
    bf16 = jnp.bfloat16

    steps = np.arange(rope_width, dtype=np.float32) % (rope_width // 2)
    frequency = np.power(np.float32(rope_base), -2.0 * steps / rope_width).astype(np.float32)[None]
    both_width = latent.shape[1] + rope_width
    broad_width = key_up_broad.shape[1]
    narrow_width = key_up_narrow.shape[1]
    width = broad_width + narrow_width
    deep = resid.shape[1]
    slice_width = up_weight.shape[1] // lines
    vmem = pl.BlockSpec(memory_space=pltpu.VMEM)
    anywhere = pl.BlockSpec(memory_space=pl.ANY)
    chunks = 5
    heads = broad_width // DB + narrow_width // DN
    _, sems = sem_layout(lines, tp, chunks, share_rows // 16)
    f32 = jnp.float32
    return pl.pallas_call(
        functools.partial(layer_kernel, sp, tp),
        out_shape=jax.ShapeDtypeStruct((share_rows, deep), bf16),
        in_specs=[vmem] * 4 + [anywhere] * 9 + [vmem] * 3 + [anywhere] * 2,
        out_specs=vmem,
        scratch_shapes=[
            pltpu.VMEM(query_broad.shape, bf16),
            pltpu.VMEM(query_narrow.shape, bf16),
            pltpu.VMEM(resid.shape, bf16),
            pltpu.VMEM(key_up_broad.shape, bf16),
            pltpu.VMEM(value_up_broad.shape, bf16),
            pltpu.VMEM(key_up_narrow.shape, bf16),
            pltpu.VMEM(value_up_narrow.shape, bf16),
            pltpu.VMEM((share_rows, both_width), bf16),
            pltpu.VMEM(query_broad.shape, bf16),
            pltpu.VMEM(query_narrow.shape, bf16),
            pltpu.VMEM((sp, tp, share_rows, both_width), bf16),
            pltpu.VMEM((heads, local_rows, 1), f32),
            pltpu.VMEM((heads, local_rows, 1), f32),
            pltpu.VMEM((heads, local_rows, lane_tile), f32),
            pltpu.VMEM((tp, share_rows, width), bf16),
            pltpu.VMEM((tp, share_rows, width), bf16),
            pltpu.VMEM(out_broad.shape, bf16),
            pltpu.VMEM(out_narrow.shape, bf16),
            pltpu.VMEM((2, sp, up_weight.shape[0], slice_width), bf16),
            pltpu.VMEM((2, lines, cols, down_weight.shape[0], slice_width), bf16),
            pltpu.VMEM((2, lines, share_rows, deep), bf16),
            pltpu.VMEM((2 * lines * share_rows, 2 * slice_width), bf16),
            pltpu.VMEM((lines, share_rows, deep), f32),
            pltpu.VMEM((lines, share_rows, deep), bf16),
            pltpu.VMEM((lines, share_rows, deep), bf16),
            pltpu.VMEM((3, share_rows, deep), bf16),
            pltpu.VMEM((2, share_rows, deep), bf16),
            pltpu.VMEM((share_rows, deep), bf16),
            pltpu.VMEM((share_rows, deep), bf16),
            pltpu.VMEM((share_rows, deep), f32),
            pltpu.SemaphoreType.DMA((2 * sems,)),
            pltpu.SemaphoreType.DMA((sems,)),
            pltpu.SemaphoreType.DMA((12,)),
            pltpu.SemaphoreType.REGULAR,
        ],
        compiler_params=pltpu.CompilerParams(
            collective_id=0, has_side_effects=True, vmem_limit_bytes=60 * 2**20
        ),
    )(
        latent,
        key_rope.T,
        frequency,
        latent_gain[None],
        query_broad,
        query_narrow,
        resid,
        key_up_broad,
        value_up_broad,
        key_up_narrow,
        value_up_narrow,
        out_broad,
        out_narrow,
        post_gain[None],
        ffn_gain[None],
        ffn_out_gain[None],
        up_weight,
        down_weight,
    )


def solution(mesh):
    in_specs = (
        P("sp", None),
        P("sp", "tp"),
        P("sp", "tp"),
        P("sp", None),
        P("sp", None),
        P(),
        P(None, "tp"),
        P(None, "tp"),
        P(None, "tp"),
        P(None, "tp"),
        P(),
        P(),
        P(),
        P(),
        P("sp", "tp"),
        P("sp", "tp"),
        P(),
    )
    out_specs = P(("sp", "tp"), None)
    sp = mesh.shape["sp"]
    tp = mesh.shape["tp"]

    def whole(*args):
        hidden = args[14].shape[1] // tp
        rows = args[0].shape[0] // sp
        lines = sp // row_parts
        fits = (
            sp % row_parts == 0
            and tp & (tp - 1) == 0
            and tp == 4
            and lines == 4
            and hidden % (lines * lane_tile) == 0
            and args[0].shape[1] % (2 * lane_tile * sp) == 0
            and rows % (16 * tp) == 0
        )
        body = fast_local if fits else local
        return jax.shard_map(
            body, mesh=mesh, in_specs=in_specs, out_specs=out_specs, check_vma=False
        )(*args)

    return whole
```

```python
import functools
import math

import jax
import jax.numpy as jnp
import numpy as np
from jax import lax
from jax.experimental import pallas as pl
from jax.experimental.pallas import tpu as pltpu
from jax.sharding import PartitionSpec as P

DB = 128
DN = 64


norm_eps = 1e-06
rope_base = 500000.0
masked_score = -1e30


def rotate(values, positions):
    full_width = values.shape[-1]
    half_width = full_width // 2
    frequency = rope_base ** (-2.0 * jnp.arange(half_width, dtype=jnp.float32) / full_width)
    angles = positions.astype(jnp.float32)[:, None] * frequency[None, :]
    angle_shape = (angles.shape[0],) + (1,) * (values.ndim - 2) + (half_width,)
    cosine = jnp.cos(angles).reshape(angle_shape)
    sine_part = jnp.sin(angles).reshape(angle_shape)
    leading = values[..., :half_width]
    trailing = values[..., half_width:]
    return jnp.concatenate(
        [leading * cosine - trailing * sine_part, trailing * cosine + leading * sine_part], axis=-1
    )


def rms_scale(values, norm_gain):
    return (
        values * lax.rsqrt(jnp.mean(values * values, axis=-1, keepdims=True) + norm_eps) * norm_gain
    )


def group_update(
    running, nope_query, rope_query, key_rows, key_rot, value_rows, score_scale, allowed
):
    old_max, old_sum, old_acc = running
    scores = jnp.einsum("qhd,khd->hqk", nope_query, key_rows, preferred_element_type=jnp.float32)
    scores = scores + jnp.einsum(
        "qhd,kd->hqk", rope_query, key_rot, preferred_element_type=jnp.float32
    )
    scores = jnp.where(allowed, scores * score_scale, masked_score)
    new_max = jnp.maximum(old_max, jnp.max(scores, axis=-1))
    exponent = jnp.where(allowed, jnp.exp(scores - new_max[:, :, None]), 0.0)
    factor = jnp.exp(old_max - new_max)
    new_sum = old_sum * factor + jnp.sum(exponent, axis=-1)
    weighted = jnp.einsum(
        "hqk,khd->qhd",
        exponent.astype(jnp.bfloat16),
        value_rows,
        preferred_element_type=jnp.float32,
    )
    new_acc = old_acc * jnp.transpose(factor)[:, :, None] + weighted
    return (new_max, new_sum, new_acc)


def local(
    resid,
    query_broad,
    query_narrow,
    latent,
    key_rope,
    latent_gain,
    key_up_broad,
    value_up_broad,
    key_up_narrow,
    value_up_narrow,
    out_broad,
    out_narrow,
    post_gain,
    ffn_gain,
    up_weight,
    down_weight,
    ffn_out_gain,
):
    local_rows = resid.shape[0]
    head_parts = lax.axis_size("tp")
    share_rows = local_rows // head_parts
    row_offset = lax.axis_index("sp") * local_rows
    last_query = row_offset + local_rows - 1
    query_pos = row_offset + jnp.arange(local_rows, dtype=jnp.int32)
    rope_width = key_rope.shape[1]
    broad_count = key_up_broad.shape[1] // DB
    narrow_count = key_up_narrow.shape[1] // DN
    broad_heads = query_broad.reshape(local_rows, broad_count, DB + rope_width)
    broad_nope = broad_heads[:, :, :DB]
    broad_rope = rotate(broad_heads[:, :, DB:].astype(jnp.float32), query_pos).astype(jnp.bfloat16)
    narrow_heads = query_narrow.reshape(local_rows, narrow_count, DN + rope_width)
    narrow_nope = narrow_heads[:, :, :DN]
    narrow_rope = rotate(narrow_heads[:, :, DN:].astype(jnp.float32), query_pos).astype(
        jnp.bfloat16
    )
    broad_scale = (DB + rope_width) ** (-0.5)
    narrow_scale = (DN + rope_width) ** (-0.5)

    def attend(running, latent_rows, rope_rows, first_row):
        key_count = latent_rows.shape[0]
        key_pos = first_row + jnp.arange(key_count, dtype=jnp.int32)
        latent_normed = rms_scale(latent_rows.astype(jnp.float32), latent_gain).astype(jnp.bfloat16)

        def expand(weight, head_size):
            product = jnp.dot(latent_normed, weight, preferred_element_type=jnp.float32)
            return product.astype(jnp.bfloat16).reshape(key_count, -1, head_size)

        key_rot = rotate(rope_rows.astype(jnp.float32), key_pos).astype(jnp.bfloat16)
        allowed = (key_pos[None, :] <= query_pos[:, None])[None]
        broad_state = group_update(
            running[0],
            broad_nope,
            broad_rope,
            expand(key_up_broad, DB),
            key_rot,
            expand(value_up_broad, DB),
            broad_scale,
            allowed,
        )
        narrow_state = group_update(
            running[1],
            narrow_nope,
            narrow_rope,
            expand(key_up_narrow, DN),
            key_rot,
            expand(value_up_narrow, DN),
            narrow_scale,
            allowed,
        )
        return (broad_state, narrow_state)

    def fresh(head_count, head_size):
        return (
            jnp.full((head_count, local_rows), masked_score, jnp.float32),
            jnp.zeros((head_count, local_rows), jnp.float32),
            jnp.zeros((local_rows, head_count, head_size), jnp.float32),
        )

    initial = (fresh(broad_count, DB), fresh(narrow_count, DN))
    latent_piece = lax.all_gather(latent, "sp", axis=0, tiled=True)
    rope_piece = lax.all_gather(key_rope, "sp", axis=0, tiled=True)
    piece_rows = latent_piece.shape[0]
    block_rows = math.gcd(piece_rows, 1024)

    def one_block(block_index, carried):
        begin = block_index * block_rows
        latent_block = lax.dynamic_slice_in_dim(latent_piece, begin, block_rows, 0)
        rope_block = lax.dynamic_slice_in_dim(rope_piece, begin, block_rows, 0)

        def unchanged(kept_state):
            return kept_state

        def updated(kept_state):
            return attend(kept_state, latent_block, rope_block, begin)

        return lax.cond(begin > last_query, unchanged, updated, carried)

    final_state = lax.fori_loop(0, piece_rows // block_rows, one_block, initial)

    def finish(running):
        run_max, run_sum, run_acc = running
        return (
            (run_acc / jnp.transpose(run_sum)[:, :, None])
            .astype(jnp.bfloat16)
            .reshape(local_rows, -1)
        )

    attn_broad = finish(final_state[0])
    attn_narrow = finish(final_state[1])
    rows_broad, rows_narrow = (
        lax.all_to_all(attn_broad, "tp", split_axis=0, concat_axis=1, tiled=True),
        lax.all_to_all(attn_narrow, "tp", split_axis=0, concat_axis=1, tiled=True),
    )
    projected = jnp.dot(rows_broad, out_broad, preferred_element_type=jnp.float32) + jnp.dot(
        rows_narrow, out_narrow, preferred_element_type=jnp.float32
    )
    own_resid = lax.dynamic_slice_in_dim(resid, lax.axis_index("tp") * share_rows, share_rows, 0)
    mixed = (own_resid.astype(jnp.float32) + rms_scale(projected, post_gain)).astype(jnp.bfloat16)
    normed = rms_scale(mixed.astype(jnp.float32), ffn_gain).astype(jnp.bfloat16)
    up_full, down_full = (
        lax.all_gather(up_weight, "sp", axis=0, tiled=True),
        lax.all_gather(down_weight, "sp", axis=0, tiled=True),
    )
    hidden = jnp.square(
        jax.nn.relu(
            jnp.dot(
                lax.all_gather(normed, "tp", axis=0, tiled=True),
                up_full,
                preferred_element_type=jnp.float32,
            )
        )
    ).astype(jnp.bfloat16)
    ffn = lax.psum_scatter(
        lax.dot_general(
            hidden, down_full, (((1,), (1,)), ((), ())), preferred_element_type=jnp.float32
        ).astype(jnp.bfloat16),
        "tp",
        scatter_dimension=0,
        tiled=True,
    ).astype(jnp.float32)
    return (mixed.astype(jnp.float32) + rms_scale(ffn, ffn_out_gain)).astype(jnp.bfloat16)

lane_tile = 128
row_parts = 2
mesh_id = pl.DeviceIdType.MESH


def sem_layout(lines, tp, chunks, row_chunks):
    sizes = {
        "lat_z": lines,
        "lat_y": lines,
        "lat_x": 2 * lines,
        "lat_c": 4 * lines,
        "up_z": lines,
        "up_y": lines,
        "up_c": 2 * lines,
        "down_z": 2 * lines,
        "down_y": 2 * lines,
        "down_c": 4 * lines,
        "heads": tp,
        "row_z": lines * row_chunks,
        "row_x": lines * row_chunks,
        "sum_x": chunks * lines,
        "sum_r": chunks * 2,
        "sum_m": chunks,
        "sum_f": chunks,
    }
    base, total = {}, 0
    for name, size in sizes.items():
        base[name] = total
        total += size
    return base, total


def layer_kernel(
    sp,
    tp,
    latent_ref,
    key_rope_ref,
    frequency_ref,
    latent_gain_ref,
    qb_hbm,
    qn_hbm,
    resid_hbm,
    kb_hbm,
    vb_hbm,
    kn_hbm,
    vn_hbm,
    ob_hbm,
    on_hbm,
    post_ref,
    gain_ref,
    last_ref,
    up_hbm,
    down_hbm,
    out_ref,
    qb_in,
    qn_in,
    resid_ref,
    kb_ref,
    vb_ref,
    kn_ref,
    vn_ref,
    mine_ref,
    qb_ref,
    qn_ref,
    lat,
    top_ref,
    sum_ref,
    acc_ref,
    attn,
    heads,
    ob,
    on,
    up,
    down,
    rows,
    hidden_ref,
    part,
    x_send,
    x_got,
    z_send,
    r_got,
    m_got,
    f_got,
    ffn_ref,
    send_sem,
    recv_sem,
    local_sem,
    pair_sem,
):
    cols = row_parts
    lines = sp // cols
    chunks = 5
    s = lax.axis_index("sp")
    t = lax.axis_index("tp")
    z = s // cols
    y = s % cols
    core = t % 2
    x = t // 2
    t_core = 2 * x + 1 - core
    t_x = 2 * (1 - x) + core
    t_both = 2 * (1 - x) + 1 - core
    s_y = z * cols + 1 - y
    half = z // 2
    mate = z + 1 - 2 * (z % 2)
    gate = 2 - half
    outer = 3 * (1 - half)
    inner = (z == 1) | (z == 2)
    edge = (z == 0) | (z == 3)
    bf16 = jnp.bfloat16
    f32 = jnp.float32
    block_rows = latent_ref.shape[0]
    share = block_rows // tp
    width = up.shape[3]
    row_step = 16
    row_chunks = share // row_step
    base, _ = sem_layout(lines, tp, chunks, row_chunks)

    def line(at):
        return (at * cols + y, t)

    peer_y, peer_x, peer_c, peer_b = (s_y, t), (s, t_x), (s, t_core), (s, t_both)
    peers = [line(mate), line(gate), line(outer), peer_y, peer_x, peer_c, peer_b]
    barrier = pltpu.get_barrier_semaphore()
    for peer in peers:
        pl.semaphore_signal(barrier, inc=1, device_id=peer, device_id_type=mesh_id)

    locals_ = []

    def bring(src, dst):
        copy = pltpu.make_async_copy(src, dst, local_sem.at[len(locals_)])
        copy.start()
        locals_.append(copy)
        return copy

    rope = key_rope_ref.shape[0]
    half_rope = rope // 2

    def table(first, count):
        row = lax.broadcasted_iota(jnp.int32, (count, rope), 0) + first
        angles = row.astype(f32) * frequency_ref[...]
        lane = lax.broadcasted_iota(jnp.int32, (count, rope), 1)
        sine = jnp.sin(angles)
        return jnp.cos(angles), jnp.where(lane < half_rope, -sine, sine)

    def turn(values, tables):
        values = values.astype(f32)
        swapped = jnp.concatenate([values[:, half_rope:], values[:, :half_rope]], axis=1)
        return (values * tables[0] + swapped * tables[1]).astype(bf16)

    latent_width = latent_ref.shape[1]
    mine_rows = pl.ds(pl.multiple_of(t * share, 16), share)
    mine_ref[:, :latent_width] = rms_scale(
        latent_ref[mine_rows, :].astype(f32), latent_gain_ref[...]
    ).astype(bf16)
    picked = lax.broadcasted_iota(jnp.int32, (share, block_rows), 1) == (
        lax.broadcasted_iota(jnp.int32, (share, block_rows), 0) + t * share
    )
    key_rows = lax.dot_general(
        jnp.where(picked, 1.0, 0.0).astype(bf16),
        key_rope_ref[...],
        (((1,), (1,)), ((), ())),
        preferred_element_type=f32,
    )
    mine_ref[:, latent_width:] = turn(key_rows, table(s * block_rows + t * share, share))
    pl.semaphore_wait(barrier, len(peers))

    started = []

    def send(src, dst, peer, recv, cond=None):
        copy = pltpu.make_async_remote_copy(
            src_ref=src,
            dst_ref=dst,
            send_sem=send_sem.at[len(started)],
            recv_sem=recv_sem.at[recv],
            device_id=peer,
            device_id_type=mesh_id,
        )
        started.append((cond, copy))
        if cond is None:
            copy.start()
        else:
            pl.when(cond)(lambda: copy.start())

    def arrive(dst, recv):
        pltpu.make_async_remote_copy(
            src_ref=dst,
            dst_ref=dst,
            send_sem=send_sem.at[0],
            recv_sem=recv_sem.at[recv],
            device_id=peer_c,
            device_id_type=mesh_id,
        ).wait_recv()

    def block(k, flipped):
        return (z - k) * cols + ((1 - y) if flipped else y)

    for k in range(lines - 1, 0, -1):
        send(mine_ref, lat.at[s, t], line(z + k), base["lat_z"] + k, z + k < lines)
    send(mine_ref, lat.at[s, t], peer_y, base["lat_y"])
    send(mine_ref, lat.at[s, t], peer_x, base["lat_x"])
    send(mine_ref, lat.at[s, t], peer_c, base["lat_c"])
    own_copy = bring(mine_ref, lat.at[s, t])

    def cut(ref, at):
        return ref.at[:, pl.ds(pl.multiple_of(at * width, width), width)]

    far = (gate, outer, mate)

    def up_at(origin, at):
        return up.at[origin, at]

    def down_at(origin, at, flipped=False):
        return down.at[origin, at, (1 - y) if flipped else y]

    def send_down(dest, cond=None):
        for i in range(2):
            send(
                down_half(cut(down_hbm, dest), i),
                down_half(down_at(core, z), i),
                line(dest),
                base["down_z"] + 2 * z + i,
                cond,
            )

    def down_half(ref, i):
        rows_half = down.shape[3] // 2
        return ref.at[pl.ds(i * rows_half, rows_half)]

    def send_up(dest, cond):
        send(cut(up_hbm, dest), up_at(core, s), line(dest), base["up_z"] + z, cond)

    send_up(mate, edge)
    for dest in far:
        send_up(dest, None if dest is not mate else inner)
    send_down(mate, inner)
    send_down(gate, z == 2)
    own = [bring(cut(up_hbm, z), up_at(core, s))]
    own.append(bring(cut(down_hbm, z), down_at(core, z)))
    queries = [bring(qb_hbm, qb_in), bring(qn_hbm, qn_in)]
    expands = [
        bring(kb_hbm, kb_ref),
        bring(vb_hbm, vb_ref),
        bring(kn_hbm, kn_ref),
        bring(vn_hbm, vn_ref),
    ]
    outs = [bring(ob_hbm, ob), bring(on_hbm, on), bring(resid_hbm, resid_ref)]
    query_table = table(s * block_rows, block_rows)
    for copy in queries:
        copy.wait()

    for queries, turned, size in ((qb_in, qb_ref, DB), (qn_in, qn_ref, DN)):
        step = size + rope
        for h in range(queries.shape[1] // step):
            middle = h * step + size
            turned[:, h * step : middle] = queries[:, h * step : middle]
            turned[:, middle : middle + rope] = turn(
                queries[:, middle : middle + rope], query_table
            )

    def when(k):
        return None if k == 0 else z >= k

    def guarded(k, body):
        if k == 0:
            body()
        else:
            pl.when(z >= k)(body)

    def lat_in_z(k):
        held = lat.at[block(k, False), t]
        guarded(k, lambda: arrive(held, base["lat_z"] + k))
        send(held, held, peer_y, base["lat_y"] + k, when(k))
        send(held, held, peer_x, base["lat_x"] + 2 * k, when(k))
        send(held, held, peer_c, base["lat_c"] + 4 * k, when(k))

    def lat_in_y(k):
        held = lat.at[block(k, True), t]
        guarded(k, lambda: arrive(held, base["lat_y"] + k))
        send(held, held, peer_x, base["lat_x"] + 2 * k + 1, when(k))
        send(held, held, peer_c, base["lat_c"] + 4 * k + 1, when(k))

    def lat_in_x(k):
        for i, flipped in enumerate((False, True)):
            held = lat.at[block(k, flipped), t_x]
            guarded(k, lambda: arrive(held, base["lat_x"] + 2 * k + i))
            send(held, held, peer_c, base["lat_c"] + 4 * k + 2 + i, when(k))

    broad = kb_ref.shape[1] // DB
    narrow = kn_ref.shape[1] // DN
    wb = DB + rope
    wn = DN + rope
    keys = cols * block_rows

    def attend(k):
        for i, flipped in enumerate((False, True)):
            arrive(lat.at[block(k, flipped), t_core], base["lat_c"] + 4 * k + i)
            arrive(lat.at[block(k, flipped), t_both], base["lat_c"] + 4 * k + 2 + i)
        both = lat[pl.ds((z - k) * cols, cols)].reshape(keys, latent_width + rope)
        normed = both[:, :latent_width]
        rot = both[:, latent_width:]

        def expand(ref):
            return jnp.dot(normed, ref[...], preferred_element_type=f32).astype(bf16)

        kb, vb, kn, vn = expand(kb_ref), expand(vb_ref), expand(kn_ref), expand(vn_ref)
        if k == 0:
            query_pos = y * block_rows + lax.broadcasted_iota(jnp.int32, (block_rows, keys), 0)
            allowed = lax.broadcasted_iota(jnp.int32, (block_rows, keys), 1) <= query_pos
        for h in range(broad + narrow):
            if h < broad:
                q = qb_ref[:, h * wb : (h + 1) * wb]
                key = jnp.concatenate([kb[:, h * DB : (h + 1) * DB], rot], axis=1)
                v = vb[:, h * DB : (h + 1) * DB]
                scale = wb ** (-0.5)
            else:
                n = h - broad
                q = qn_ref[:, n * wn : (n + 1) * wn]
                key = jnp.concatenate([kn[:, n * DN : (n + 1) * DN], rot], axis=1)
                v = vn
                scale = wn ** (-0.5)
            score = scale * lax.dot_general(
                q, key, (((1,), (1,)), ((), ())), preferred_element_type=f32
            )
            if k == 0:
                score = jnp.where(allowed, score, masked_score)
                new_max = jnp.max(score, axis=-1, keepdims=True)
                e = jnp.where(allowed, jnp.exp(score - new_max), 0.0)
                new_sum = jnp.sum(e, axis=-1, keepdims=True)
                acc_ref[h] = jnp.dot(e.astype(bf16), v, preferred_element_type=f32)
            else:
                old_max = top_ref[h]
                new_max = jnp.maximum(old_max, jnp.max(score, axis=-1, keepdims=True))
                e = jnp.exp(score - new_max)
                factor = jnp.exp(old_max - new_max)
                new_sum = sum_ref[h] * factor + jnp.sum(e, axis=-1, keepdims=True)
                acc_ref[h] = acc_ref[h] * factor + jnp.dot(
                    e.astype(bf16), v, preferred_element_type=f32
                )
            top_ref[h] = new_max
            sum_ref[h] = new_sum

    def up_in_z(i, at):
        held = up_at(core, at * cols + y)
        arrive(held, base["up_z"] + at)
        send(held, held, peer_y, base["up_y"] + 1 + i)
        send(held, held, peer_c, base["up_c"] + 1 + i)

    def down_in_z(at, cond=None):
        for i in range(2):
            held = down_half(down_at(core, at), i)
            if cond is None:
                arrive(held, base["down_z"] + 2 * at + i)
            else:
                pl.when(cond)(lambda: arrive(held, base["down_z"] + 2 * at + i))
            send(held, held, peer_y, base["down_y"] + 2 * at + i, cond)
            send(held, held, peer_c, base["down_c"] + 4 * at + i, cond)

    lat_in_y(0)
    lat_in_z(1)
    lat_in_z(2)
    lat_in_z(3)
    lat_in_x(0)
    send(cut(up_hbm, z), up_at(core, s), peer_y, base["up_y"])
    send(cut(up_hbm, z), up_at(core, s), peer_c, base["up_c"])
    own_copy.wait()
    for copy in expands:
        copy.wait()
    attend(0)
    lat_in_y(1)
    lat_in_y(2)
    lat_in_y(3)
    lat_in_x(1)
    up_in_z(2, mate)
    for i in range(2):
        held = down_half(cut(down_hbm, z), i)
        own_half = down_half(down_at(core, z), i)
        send(held, own_half, peer_y, base["down_y"] + 2 * z + i)
        send(held, own_half, peer_c, base["down_c"] + 4 * z + i)
    guarded(1, lambda: attend(1))
    lat_in_x(2)
    lat_in_x(3)
    guarded(2, lambda: attend(2))
    guarded(3, lambda: attend(3))

    parts = [acc_ref[h] / sum_ref[h] for h in range(broad + narrow)]
    for h in range(broad):
        for i in range(tp):
            attn[i, :, h * DB : (h + 1) * DB] = parts[h][i * share : (i + 1) * share].astype(bf16)
    column = lax.broadcasted_iota(jnp.int32, parts[broad].shape, 1)
    merged = parts[broad]
    for n in range(1, narrow):
        merged = jnp.where(column >= n * DN, parts[broad + n], merged)
    for i in range(tp):
        attn[i, :, broad * DB :] = merged[i * share : (i + 1) * share].astype(bf16)

    turned_to = ((t_x, peer_x), (t_both, peer_b), (t_core, peer_c))
    for i, (at, peer) in enumerate(turned_to):
        send(attn.at[at], heads.at[t], peer, base["heads"] + i)
    heads[t] = attn[t]
    for copy in outs:
        copy.wait()
    for i, (at, _) in enumerate(turned_to):
        arrive(heads.at[at], base["heads"] + i)

    down_in_z(mate, edge)
    broad_width = kb_ref.shape[1]
    narrow_width = kn_ref.shape[1]
    projected = jnp.zeros((share, ob.shape[1]), f32)
    for i in range(tp):
        projected = projected + jnp.dot(
            heads[i, :, :broad_width],
            ob[i * broad_width : (i + 1) * broad_width],
            preferred_element_type=f32,
        )
        projected = projected + jnp.dot(
            heads[i, :, broad_width:],
            on[i * narrow_width : (i + 1) * narrow_width],
            preferred_element_type=f32,
        )
    mixed = (
        resid_ref[pl.ds(pl.multiple_of(t * share, 16), share), :].astype(f32)
        + rms_scale(projected, post_ref[...])
    ).astype(bf16)
    rows[0, z] = rms_scale(mixed.astype(f32), gain_ref[...]).astype(bf16)

    def row_piece(side, at, c):
        return rows.at[side, at, pl.ds(c * row_step, row_step)]

    crossing = []
    for dest in (gate, mate):
        for c in range(row_chunks):
            held = row_piece(0, z, c)
            send(held, held, line(dest), base["row_z"] + z * row_chunks + c)
            if dest is gate:
                crossing.append(started.pop()[1])
                started.append((edge, crossing[-1]))
                send(held, row_piece(1, z, c), peer_x, base["row_x"] + c)
    send_down(mate, edge)
    send_down(gate, z == 3)

    def up_in_y(i, at):
        held = up_at(core, at * cols + 1 - y)
        arrive(held, base["up_y"] + i)
        send(held, held, peer_c, base["up_c"] + lines + i)

    def row_in(i, at):
        for c in range(row_chunks):
            held = row_piece(0, at, c)
            index = base["row_z"] + at * row_chunks + c
            arrive(held, index)
            if i < 2:
                send(held, held, line(mate), index, inner)
            send(held, row_piece(1, at, c), peer_x, base["row_x"] + (1 + i) * row_chunks + c)

    up_in_z(0, gate)
    up_in_z(1, outer)
    row_in(2, mate)
    row_in(0, gate)
    row_in(1, outer)
    @pl.when(inner)
    def _():
        for copy in crossing:
            copy.wait_send()
        pl.semaphore_signal(pair_sem, inc=1, device_id=peer_c, device_id_type=mesh_id)
        pl.semaphore_wait(pair_sem, 1)

    send_down(gate, z == 1)
    send_down(outer, inner)
    steps = (z,) + far
    down_in_z(mate, inner)
    down_in_z(gate, edge)
    send_down(gate, z == 0)
    send_down(outer, edge)
    for i, at in enumerate(steps):
        up_in_y(i, at)
    own[0].wait()
    for i, at in enumerate(steps):
        arrive(up_at(1 - core, at * cols + y), base["up_c"] + i)
        arrive(up_at(1 - core, at * cols + 1 - y), base["up_c"] + lines + i)

    deep = sp * up.shape[2]

    def raise_rows(j):
        block_in = rows[j].reshape(lines * share, rows.shape[3])
        for origin in range(2):
            product = jnp.dot(
                block_in, up[origin].reshape(deep, width), preferred_element_type=f32
            )
            hidden_ref[
                j * lines * share : (j + 1) * lines * share, origin * width : (origin + 1) * width
            ] = jnp.square(jnp.maximum(product, 0.0)).astype(bf16)

    raise_rows(0)

    def down_in_y(at):
        for i in range(2):
            held = down_half(down_at(core, at, True), i)
            arrive(held, base["down_y"] + 2 * at + i)
            send(held, held, peer_c, base["down_c"] + 4 * at + 2 + i)

    units = (outer, gate, mate, z)

    deep_part = down.shape[3]
    early = (lines - 1) * half
    late = (lines - 1) * (1 - half)

    def sibling_in(at, flipped):
        for i in range(2):
            held = down_half(down_at(1 - core, at, flipped), i)
            arrive(held, base["down_c"] + 4 * at + 2 * flipped + i)

    def columns_of(start, count):
        if not isinstance(start, int):
            start = pl.multiple_of(start, lane_tile)
        return pl.ds(start, count)

    def lower(weights, columns):
        total = None
        for origin in range(2):
            product = lax.dot_general(
                hidden_ref[:, origin * width : (origin + 1) * width],
                weights(origin),
                (((1,), (1,)), ((), ())),
                preferred_element_type=f32,
            )
            total = product if total is None else total + product
        total = total.reshape(2, lines, share, total.shape[1])
        part[:, :, columns] = total[0]
        x_send[:, :, columns] = total[1].astype(bf16)

    def send_sums(group, columns):
        for i, at in enumerate(units):
            send(
                x_send.at[at, :, columns],
                x_got.at[at, :, columns],
                peer_x,
                base["sum_x"] + group * lines + i,
            )

    def lower_middle():
        for at in (1, 2):
            sibling_in(at, 0)
            sibling_in(at, 1)
        wide = 2 * cols * deep_part
        columns = pl.ds(cols * deep_part, wide)
        lower(lambda origin: down[origin, 1:3].reshape(wide, width), columns)
        send_sums(0, columns)
        return 0, columns

    def lower_edge(at, flipped):
        sibling_in(at, flipped)
        side = (1 - y) if flipped else y
        columns = columns_of((at * cols + side) * deep_part, deep_part)
        lower(lambda origin: down[origin, at, side], columns)
        group = 1 + 2 * (at // (lines - 1)) + flipped
        send_sums(group, columns)
        return group, columns

    def pair(group, columns, i):
        at = units[i]
        arrive(x_got.at[at, :, columns], base["sum_x"] + group * lines + i)
        return part[at, :, columns] + x_got[at, :, columns].astype(f32)

    def sum_copy(i, got, peer, index, cond, columns):
        copy = pltpu.make_async_remote_copy(
            src_ref=z_send.at[i, :, columns],
            dst_ref=got.at[:, columns],
            send_sem=send_sem.at[len(started)],
            recv_sem=recv_sem.at[index],
            device_id=peer,
            device_id_type=mesh_id,
        )
        started.append((cond, copy))
        return copy

    def combine(group, columns):
        near = [
            sum_copy(
                i, r_got.at[i], line(mate), base["sum_r"] + group * 2 + i, edge, columns
            )
            for i in range(2)
        ]
        own_sum = sum_copy(2, m_got, line(mate), base["sum_m"] + group, None, columns)
        across = [
            sum_copy(i, f_got, line(units[i]), base["sum_f"] + group, inner, columns)
            for i in range(2)
        ]

        def mate_part():
            z_send[2, :, columns] = pair(group, columns, 2).astype(bf16)
            own_sum.start()

        def edge_part():
            for i in range(2):
                z_send[i, :, columns] = pair(group, columns, i).astype(bf16)
                near[i].start()
            mate_part()

        def inner_part():
            for i in range(2):
                value = pair(group, columns, i)
                got = r_got.at[i, :, columns]
                arrive(got, base["sum_r"] + group * 2 + i)
                z_send[i, :, columns] = (value + got[...].astype(f32)).astype(bf16)
                across[i].start()
            mate_part()

        return edge_part, inner_part

    def finish(group, columns):
        value = pair(group, columns, 3)
        arrive(m_got.at[:, columns], base["sum_m"] + group)
        value = value + m_got[:, columns].astype(f32)
        arrive(f_got.at[:, columns], base["sum_f"] + group)
        ffn_ref[:, columns] = value + f_got[:, columns].astype(f32)

    for i, at in enumerate((z, gate, outer, mate)):
        for c in range(row_chunks):
            arrive(row_piece(1, at, c), base["row_x"] + i * row_chunks + c)
    raise_rows(1)
    own[1].wait()
    down_in_y(early)
    made = [lower_edge(early, 0), lower_edge(early, 1)]
    down_in_z(gate, inner)
    down_in_y(1)
    down_in_y(2)
    made.append(lower_middle())
    steps_of = [combine(*item) for item in made]
    pl.when(edge)(steps_of[0][0])
    pl.when(edge)(steps_of[1][0])
    down_in_z(outer)
    made.append(lower_edge(late, 0))
    steps_of.append(combine(*made[3]))
    pl.when(edge)(steps_of[2][0])
    down_in_y(late)
    made.append(lower_edge(late, 1))
    steps_of.append(combine(*made[4]))
    for item in steps_of[:3]:
        pl.when(inner)(item[1])
    for item in steps_of[3:]:
        pl.when(edge)(item[0])
        pl.when(inner)(item[1])
    finish(*made[2])
    for at, flipped in ((early, 0), (early, 1), (late, 0), (late, 1)):
        side = (1 - y) if flipped else y
        finish(
            1 + 2 * (at // (lines - 1)) + flipped,
            columns_of((at * cols + side) * deep_part, deep_part),
        )
    out_ref[...] = (mixed.astype(f32) + rms_scale(ffn_ref[...], last_ref[...])).astype(bf16)
    for cond, copy in started:
        if cond is None:
            copy.wait_send()
        else:
            pl.when(cond)(lambda: copy.wait_send())


def fast_local(
    resid,
    query_broad,
    query_narrow,
    latent,
    key_rope,
    latent_gain,
    key_up_broad,
    value_up_broad,
    key_up_narrow,
    value_up_narrow,
    out_broad,
    out_narrow,
    post_gain,
    ffn_gain,
    up_weight,
    down_weight,
    ffn_out_gain,
):
    sp = lax.axis_size("sp")
    tp = lax.axis_size("tp")
    cols = row_parts
    lines = sp // cols
    local_rows = resid.shape[0]
    share_rows = local_rows // tp
    rope_width = key_rope.shape[1]
    bf16 = jnp.bfloat16

    steps = np.arange(rope_width, dtype=np.float32) % (rope_width // 2)
    frequency = np.power(np.float32(rope_base), -2.0 * steps / rope_width).astype(np.float32)[None]
    both_width = latent.shape[1] + rope_width
    broad_width = key_up_broad.shape[1]
    narrow_width = key_up_narrow.shape[1]
    width = broad_width + narrow_width
    deep = resid.shape[1]
    slice_width = up_weight.shape[1] // lines
    vmem = pl.BlockSpec(memory_space=pltpu.VMEM)
    anywhere = pl.BlockSpec(memory_space=pl.ANY)
    chunks = 5
    heads = broad_width // DB + narrow_width // DN
    _, sems = sem_layout(lines, tp, chunks, share_rows // 16)
    f32 = jnp.float32
    return pl.pallas_call(
        functools.partial(layer_kernel, sp, tp),
        out_shape=jax.ShapeDtypeStruct((share_rows, deep), bf16),
        in_specs=[vmem] * 4 + [anywhere] * 9 + [vmem] * 3 + [anywhere] * 2,
        out_specs=vmem,
        scratch_shapes=[
            pltpu.VMEM(query_broad.shape, bf16),
            pltpu.VMEM(query_narrow.shape, bf16),
            pltpu.VMEM(resid.shape, bf16),
            pltpu.VMEM(key_up_broad.shape, bf16),
            pltpu.VMEM(value_up_broad.shape, bf16),
            pltpu.VMEM(key_up_narrow.shape, bf16),
            pltpu.VMEM(value_up_narrow.shape, bf16),
            pltpu.VMEM((share_rows, both_width), bf16),
            pltpu.VMEM(query_broad.shape, bf16),
            pltpu.VMEM(query_narrow.shape, bf16),
            pltpu.VMEM((sp, tp, share_rows, both_width), bf16),
            pltpu.VMEM((heads, local_rows, 1), f32),
            pltpu.VMEM((heads, local_rows, 1), f32),
            pltpu.VMEM((heads, local_rows, lane_tile), f32),
            pltpu.VMEM((tp, share_rows, width), bf16),
            pltpu.VMEM((tp, share_rows, width), bf16),
            pltpu.VMEM(out_broad.shape, bf16),
            pltpu.VMEM(out_narrow.shape, bf16),
            pltpu.VMEM((2, sp, up_weight.shape[0], slice_width), bf16),
            pltpu.VMEM((2, lines, cols, down_weight.shape[0], slice_width), bf16),
            pltpu.VMEM((2, lines, share_rows, deep), bf16),
            pltpu.VMEM((2 * lines * share_rows, 2 * slice_width), bf16),
            pltpu.VMEM((lines, share_rows, deep), f32),
            pltpu.VMEM((lines, share_rows, deep), bf16),
            pltpu.VMEM((lines, share_rows, deep), bf16),
            pltpu.VMEM((3, share_rows, deep), bf16),
            pltpu.VMEM((2, share_rows, deep), bf16),
            pltpu.VMEM((share_rows, deep), bf16),
            pltpu.VMEM((share_rows, deep), bf16),
            pltpu.VMEM((share_rows, deep), f32),
            pltpu.SemaphoreType.DMA((2 * sems,)),
            pltpu.SemaphoreType.DMA((sems,)),
            pltpu.SemaphoreType.DMA((12,)),
            pltpu.SemaphoreType.REGULAR,
        ],
        compiler_params=pltpu.CompilerParams(
            collective_id=0, has_side_effects=True, vmem_limit_bytes=60 * 2**20
        ),
    )(
        latent,
        key_rope.T,
        frequency,
        latent_gain[None],
        query_broad,
        query_narrow,
        resid,
        key_up_broad,
        value_up_broad,
        key_up_narrow,
        value_up_narrow,
        out_broad,
        out_narrow,
        post_gain[None],
        ffn_gain[None],
        ffn_out_gain[None],
        up_weight,
        down_weight,
    )


def solution(mesh):
    in_specs = (
        P("sp", None),
        P("sp", "tp"),
        P("sp", "tp"),
        P("sp", None),
        P("sp", None),
        P(),
        P(None, "tp"),
        P(None, "tp"),
        P(None, "tp"),
        P(None, "tp"),
        P(),
        P(),
        P(),
        P(),
        P("sp", "tp"),
        P("sp", "tp"),
        P(),
    )
    out_specs = P(("sp", "tp"), None)
    sp = mesh.shape["sp"]
    tp = mesh.shape["tp"]

    def whole(*args):
        hidden = args[14].shape[1] // tp
        rows = args[0].shape[0] // sp
        lines = sp // row_parts
        fits = (
            sp % row_parts == 0
            and tp & (tp - 1) == 0
            and tp == 4
            and lines == 4
            and hidden % (lines * lane_tile) == 0
            and args[0].shape[1] % (2 * lane_tile * sp) == 0
            and rows % (16 * tp) == 0
        )
        body = fast_local if fits else local
        return jax.shard_map(
            body, mesh=mesh, in_specs=in_specs, out_specs=out_specs, check_vma=False
        )(*args)

    return whole
```
